512 devices in a mesh: sp: 32 (over z, core), tp: 16 (over y, x).
Axes of the slice: x: 4, y: 4, z: 16, core: 2. Of those that a mesh axis runs over, the one named last changes fastest.
Arguments:
- residual_in: bfloat16 [8192, 2048], P('sp'), may hold values from -3 to 3
- mix_gain: float32 [2048], replicated, may hold values from 0.1 to 1.9
- pool_weight: bfloat16 [512, 2048], P(None, 'tp'), may hold values from -0.5 to 0.5
- pool_scale: float32 [2048], P('tp'), may hold values from 0.1 to 1.9
- ffn_gain: float32 [2048], replicated, may hold values from 0.1 to 1.9
- route_ids: int32 [8192, 2], P('sp'), may hold values from 0 to 31, all different within a row; in each aligned block of 16 rows (0 to 15, 16 to 31, ...) at most 2 rows name the same one
- route_weights: float32 [8192, 2], P('sp'), may hold values from 0.1 to 1
- gate_weight: bfloat16 [32, 2048, 3584], P('sp', None, 'tp'), may hold values from -0.125 to 0.125
- up_weight: bfloat16 [32, 2048, 3584], P('sp', None, 'tp'), may hold values from -0.125 to 0.125
- down_weight: bfloat16 [32, 3584, 2048], P('sp', 'tp'), may hold values from -0.09375 to 0.09375
Outputs:
- layer_out: bfloat16 [8192, 2048], P('sp')
The draws below stay inside these ranges and needn't reach their ends.
Inputs may be any that keep to these rules, and one draw needn't show every extreme that they name: `route_ids`: each row names 2 different experts; in each aligned block of 16 rows no expert is named by more than 2 rows, and some block has an expert named by exactly 2 rows.
All inputs are finite; a program needn't handle non-finite values.
Results may differ from the reference program's by a relative error of at most 0.0074.
Values may be sent and summed in bfloat16 or wider, within the bound.
No kernel may reach another device: no remote copies, remote signals or barrier semaphores. Data moves between devices by JAX's collectives and lax.ppermute only.
A program may use at most 64 MiB of HBM per device.

```python
import math
import jax
import jax.numpy as jnp
import numpy as np
from jax import lax

D = 2048
GROUPS = 4
SPAN = 16
C = 512
FF_EXP = 3584
TOP_K = 2
EXPERTS = 32
ROWS = 16
CAP = 2
TOKENS = 8192
N_TP = 16


def level_of(rng, shape, split, smallest, top_value):
    def one(dim, parts):
        draws = jax.random.uniform(jax.random.fold_in(jax.random.fold_in(rng, 6), dim), (parts,), jnp.float32, smallest / len(split), top_value / len(split))
        return jnp.repeat(jnp.exp(draws), shape[dim] // parts).reshape((-1,) + (1,) * (len(shape) - dim - 1))

    factor_of = one(*split[0])
    for cut in split[1:]:
        factor_of = factor_of * one(*cut)
    return factor_of


def deal_out(key, own, number, rows, number_of, top, most, lean):
    sequence = jax.random.permutation(key, number_of)
    heavy_load, ordinary = shares(number_of, rows * top, most, lean, True), shares(number_of, rows * top, most, lean, False)
    places = jnp.arange(number_of)

    def named(sizes, offset_by):
        used = int((sizes > 0).sum())
        fixed = max(1, used // 4)
        passed = fixed + (places - fixed + offset_by * (used - fixed)) % max(1, number_of - fixed)
        return jnp.zeros((number_of,), jnp.int32).at[sequence[jnp.where(places < fixed, places, passed)]].set(jnp.asarray(sizes, jnp.int32))

    sizes = jnp.where(number % 4 == 0, named(heavy_load, number // 4), named(ordinary, number - number // 4 - 1))
    mixed = jax.random.permutation(jax.random.fold_in(own, 3), number_of)
    source_of, receiver = mixed[0:number_of // 2 * 2:2], mixed[1:number_of // 2 * 2:2]
    room = jnp.minimum(sizes[source_of] - 1, most - sizes[receiver]) // 2
    room = jnp.where((source_of == sequence[0]) | (receiver == sequence[0]) | (sizes[receiver] == 0), 0, jnp.maximum(room, 0))
    passed = jax.random.randint(jax.random.fold_in(own, 4), (number_of // 2,), 0, 1 << 20) % (room + 1)
    sizes = sizes.at[source_of].add(-passed).at[receiver].add(passed)
    items = jnp.searchsorted(jnp.cumsum(sizes), jnp.arange(rows * top), side="right").astype(jnp.int32)
    table = items.reshape(top, rows).T
    table = table[jax.random.permutation(jax.random.fold_in(own, 1), rows)]
    offset_by = jax.random.randint(jax.random.fold_in(own, 2), (rows, 1), 0, top)
    return jnp.take_along_axis(table, (jnp.arange(top)[None, :] + offset_by) % top, axis=1)


def shares(number_of, total, bound, lean, full):
    loads = [(1 << 20) // math.isqrt(standing ** lean) + 1 for standing in range(1, number_of + 1)]
    largest = bound if full else min(bound, max(-(-total // number_of), total * loads[0] // sum(loads)))
    least = 1 if total - largest >= number_of - 1 else 0
    counts, surplus = [largest] + [least] * (number_of - 1), total - largest - least * (number_of - 1)
    while surplus > 0:
        movable = [i for i in range(1, number_of) if counts[i] < largest] or [i for i in range(1, number_of) if counts[i] < bound]
        pool, remaining = sum([loads[i] for i in movable]), surplus
        for i in movable:
            extra = min(bound - counts[i], max(1, remaining * loads[i] // pool), surplus)
            counts[i] = counts[i] + extra
            surplus = surplus - extra
    return np.array(counts)


def gaussian(stream_key, shape, deviation, most, cuts=(), held_as=jnp.bfloat16):
    result = jax.random.normal(stream_key, shape, jnp.float32) * deviation
    if len(cuts) > 0:
        result = level_of(stream_key, shape, cuts, -0.22, 0.18) * result
    return jnp.clip(result, min=-most, max=most).astype(held_as)


def setup_inputs(seed: int = 0) -> dict:
    streams_of = jax.random.split(jax.random.key(seed), 11)
    residual_in = gaussian(streams_of[0], (TOKENS, D), 0.5, 3.0, ((0, 32),))
    mix_gain = jnp.clip(1.0 + 0.18 * jax.random.normal(streams_of[1], (D,), jnp.float32), 0.1, 1.9)
    pool_weight = gaussian(streams_of[2], (C, D), (C // 4) ** -0.5, 0.5, ((1, 16),))
    pool_scale = jnp.clip(1.0 + 0.18 * jax.random.normal(streams_of[3], (D,), jnp.float32), 0.1, 1.9)
    ffn_gain = jnp.clip(1.0 + 0.18 * jax.random.normal(streams_of[4], (D,), jnp.float32), 0.1, 1.9)
    route_ids_keys = jax.random.split(jax.random.fold_in(streams_of[5], 1), TOKENS // ROWS)
    route_ids_turns = jax.random.permutation(jax.random.fold_in(streams_of[5], 3), TOKENS // ROWS)
    route_ids = jax.vmap(lambda own, number: deal_out(jax.random.fold_in(streams_of[5], 2), own, number, ROWS, EXPERTS, TOP_K, CAP, 2))(route_ids_keys, route_ids_turns).reshape((TOKENS, TOP_K))
    route_weights = jnp.clip(jnp.exp(math.log(1.0) - 2.3025851 * jax.random.uniform(streams_of[6], (TOKENS, TOP_K), jnp.float32) ** level_of(streams_of[6], (TOKENS, TOP_K), ((0, 32),), -0.2, 0.2)), 0.1, 1.0)
    gate_weight = gaussian(streams_of[7], (EXPERTS, D, FF_EXP), D ** -0.5, 0.125, ((0, 32), (2, 16)))
    up_weight = gaussian(streams_of[8], (EXPERTS, D, FF_EXP), D ** -0.5, 0.125, ((0, 32), (2, 16)))
    down_weight = gaussian(streams_of[9], (EXPERTS, FF_EXP, D), FF_EXP ** -0.5, 0.09375, ((0, 32), (1, 16)))
    return {"residual_in": residual_in, "mix_gain": mix_gain, "pool_weight": pool_weight, "pool_scale": pool_scale, "ffn_gain": ffn_gain, "route_ids": route_ids, "route_weights": route_weights, "gate_weight": gate_weight, "up_weight": up_weight, "down_weight": down_weight}


EPS = 1e-06

def rms_scale(values, gain):
    return values * lax.rsqrt(lax.optimization_barrier(jnp.mean(values * values, axis=-1, keepdims=True)) + EPS) * gain

def reference(residual_in, mix_gain, pool_weight, pool_scale, ffn_gain, route_ids, route_weights, gate_weight, up_weight, down_weight):
    stream = residual_in.astype(jnp.float32)
    normed_in = rms_scale(stream, mix_gain).astype(jnp.bfloat16)
    shifted_in = jnp.concatenate([jnp.zeros((SPAN, D), jnp.bfloat16), normed_in], axis=0).astype(jnp.float32)
    position = jnp.arange(TOKENS, dtype=jnp.int32)
    pieces = []
    for group_index in range(GROUPS):
        window = 2 ** (group_index + 1)
        first = group_index * C
        window_sum = jnp.zeros((TOKENS, C), jnp.float32)
        for offset in range(window):
            window_sum = window_sum + shifted_in[SPAN - offset:SPAN - offset + TOKENS, first:first + C]
        divisor = jnp.minimum(position + 1, window).astype(jnp.float32)
        pieces.append(window_sum / divisor[:, None] - shifted_in[SPAN:, first:first + C])
    pooled = jnp.concatenate(pieces, axis=1).astype(jnp.bfloat16)
    mapped = jnp.concatenate([jnp.dot(pooled[:, g * C:(g + 1) * C], pool_weight[:, g * C:(g + 1) * C], preferred_element_type=jnp.float32) for g in range(GROUPS)], axis=1)
    mixer_out = (mapped * pool_scale).astype(jnp.bfloat16)
    after_mixer = (stream + mixer_out.astype(jnp.float32)).astype(jnp.bfloat16)
    normed = rms_scale(after_mixer.astype(jnp.float32), ffn_gain).astype(jnp.bfloat16)
    block_count = TOKENS // ROWS
    grouped = route_ids.reshape(block_count, ROWS * TOP_K)
    matches = (grouped[:, :, None] == jnp.arange(EXPERTS, dtype=jnp.int32)[None, None, :]).astype(jnp.int32)
    before = jnp.cumsum(matches, axis=1) - matches
    slot_of = lax.optimization_barrier(jnp.sum(before * matches, axis=-1))
    target = grouped * (block_count * CAP) + jnp.arange(block_count, dtype=jnp.int32)[:, None] * CAP + slot_of
    target = target.reshape(-1).astype(jnp.int32)
    source = (jnp.arange(TOKENS * TOP_K, dtype=jnp.int32) // TOP_K).astype(jnp.int32)
    holder = jnp.zeros((EXPERTS * block_count * CAP,), jnp.int32).at[target].set(source)
    share = FF_EXP // N_TP

    def run_expert(operands):
        indices, gate_matrix, up_matrix, down_matrix = operands
        chosen = normed[indices]
        gate_part = jnp.dot(chosen, gate_matrix, preferred_element_type=jnp.float32)
        up_part = jnp.dot(chosen, up_matrix, preferred_element_type=jnp.float32)
        hidden = (jax.nn.silu(gate_part) * up_part).astype(jnp.bfloat16)
        total = jnp.zeros((indices.shape[0], D), jnp.float32)
        for piece in range(N_TP):
            partial_value = jnp.dot(hidden[:, piece * share:(piece + 1) * share], down_matrix[piece * share:(piece + 1) * share], preferred_element_type=jnp.float32)
            total = total + partial_value.astype(jnp.bfloat16).astype(jnp.float32)
        return total.astype(jnp.bfloat16)
    outputs = lax.map(run_expert, (holder.reshape(EXPERTS, block_count * CAP), gate_weight, up_weight, down_weight))
    picked = outputs.reshape(-1, D)[target].astype(jnp.float32).reshape(TOKENS, TOP_K, D)
    expert_mix = lax.optimization_barrier(jnp.sum(route_weights[:, :, None] * picked, axis=1))
    return (after_mixer.astype(jnp.float32) + expert_mix).astype(jnp.bfloat16)
```

```python
import math

import jax
import jax.numpy as jnp
import numpy as np
from jax import lax
from jax.sharding import Mesh
from jax.sharding import PartitionSpec as P

GROUPS = 4
SPAN = 16
TOP_K = 2
SP = ("z", "c")
TP = ("y", "x")
ALL = ("z", "c", "y", "x")


EPS = 1e-06


def from_behind(value, axis, steps):
    count = lax.axis_size(axis)
    first, last = (max(0, -steps), min(count, count - steps))
    return lax.ppermute(value, axis, [(source, source + steps) for source in range(first, last)])


def rms_scale(values, gain):
    return values * lax.rsqrt(jnp.mean(values * values, axis=-1, keepdims=True) + EPS) * gain


def plane_groups(swapped):
    sizes = [lax.axis_size(a) for a in ALL]
    index = np.arange(math.prod(sizes)).reshape(sizes)
    groups = []
    for z in range(sizes[0]):
        for c in range(sizes[1]):
            plane = index[z, c]
            groups += (plane if (c % 2 == 0) != swapped else plane.T).tolist()
    return groups


def exchange(blocks, groups):
    return lax.all_to_all(blocks, ALL, 0, 0, tiled=True, axis_index_groups=groups)


def gather_stage(rows, groups):
    blocks = jnp.broadcast_to(rows[None], (len(groups[0]), *rows.shape))
    return exchange(blocks, groups).reshape(-1, rows.shape[-1])


def sum_stage(rows, groups):
    blocks = exchange(rows.reshape(len(groups[0]), -1, rows.shape[-1]), groups)
    return jnp.sum(blocks.astype(jnp.float32), axis=0).astype(jnp.bfloat16)


def slot_table(chosen_ids, experts, capacity):
    flat_ids = chosen_ids.reshape(-1)
    matches = (flat_ids[:, None] == jnp.arange(experts, dtype=jnp.int32)[None, :]).astype(jnp.int32)
    before = jnp.cumsum(matches, axis=0) - matches
    slot_of = jnp.sum(before * matches, axis=1)
    target = flat_ids * capacity + slot_of
    table = target[:, None] == jnp.arange(experts * capacity, dtype=jnp.int32)[None, :]
    return table.astype(jnp.float32).reshape(*chosen_ids.shape, experts * capacity)


def shards(
    residual_in,
    mix_gain,
    pool_weight,
    pool_scale,
    ffn_gain,
    route_ids,
    route_weights,
    gate_weight,
    up_weight,
    down_weight,
):
    tp_count = lax.axis_size(TP)
    sp_count = lax.axis_size(SP)
    tp_index = lax.axis_index(TP)
    tok_count, width = residual_in.shape
    group_width = width // GROUPS
    col_count = pool_weight.shape[1]
    row_count = tok_count // tp_count
    capacity = 2 * TOP_K * row_count // sp_count
    group_index = tp_index * col_count // group_width
    window = jnp.power(2, group_index + 1)
    stream = residual_in.astype(jnp.float32)
    inverse = lax.rsqrt(jnp.mean(stream * stream, axis=-1, keepdims=True) + EPS)
    stream_group = lax.dynamic_slice_in_dim(stream, group_index * group_width, group_width, 1)
    gain_group = lax.dynamic_slice_in_dim(mix_gain, group_index * group_width, group_width, 0)
    normed_group = (stream_group * inverse * gain_group).astype(jnp.bfloat16)
    rim_rows = from_behind(normed_group[tok_count - SPAN :], SP, 1)
    extended = jnp.concatenate([rim_rows, normed_group], axis=0).astype(jnp.float32)
    window_sum = jnp.zeros((tok_count, group_width), jnp.float32)
    for offset in range(SPAN):
        window_sum = window_sum + jnp.where(
            offset < window, extended[SPAN - offset : SPAN - offset + tok_count], 0.0
        )
    position = lax.axis_index(SP) * tok_count + jnp.arange(tok_count, dtype=jnp.int32)
    divisor = jnp.minimum(position + 1, window).astype(jnp.float32)
    pooled = (window_sum / divisor[:, None] - extended[SPAN:]).astype(jnp.bfloat16)
    mixed = (jnp.dot(pooled, pool_weight, preferred_element_type=jnp.float32) * pool_scale).astype(
        jnp.bfloat16
    )
    stream_own = lax.dynamic_slice_in_dim(stream, tp_index * row_count, row_count, 0)
    mixed_own = lax.all_to_all(mixed, TP, split_axis=0, concat_axis=1, tiled=True)
    after_own = (stream_own + mixed_own.astype(jnp.float32)).astype(jnp.bfloat16)
    normed_own = rms_scale(after_own.astype(jnp.float32), ffn_gain).astype(jnp.bfloat16)
    ids_own = lax.dynamic_slice_in_dim(route_ids, tp_index * row_count, row_count, 0)
    table_own = slot_table(ids_own, sp_count, capacity)
    outgoing = lax.dot_general(
        jnp.sum(table_own, axis=1).astype(jnp.bfloat16),
        normed_own,
        (((0,), (0,)), ((), ())),
        preferred_element_type=jnp.float32,
    )
    outgoing = outgoing.astype(jnp.bfloat16).reshape(sp_count, capacity, width)
    arrived = lax.all_to_all(outgoing, SP, split_axis=0, concat_axis=0, tiled=True)
    first, second = (plane_groups(False), plane_groups(True))
    flat_rows = gather_stage(gather_stage(arrived.reshape(-1, width), first), second)
    gate_part = jnp.dot(flat_rows, gate_weight[0], preferred_element_type=jnp.float32)
    up_part = jnp.dot(flat_rows, up_weight[0], preferred_element_type=jnp.float32)
    hidden = (jax.nn.silu(gate_part) * up_part).astype(jnp.bfloat16)
    term = jnp.dot(hidden, down_weight[0], preferred_element_type=jnp.float32).astype(jnp.bfloat16)
    expert_out = sum_stage(sum_stage(term, second), first)
    returned_rows = lax.all_to_all(
        expert_out.reshape(sp_count, capacity, width), SP, split_axis=0, concat_axis=0, tiled=True
    )
    weights_own = lax.dynamic_slice_in_dim(route_weights, tp_index * row_count, row_count, 0)
    weight_table = jnp.sum(weights_own[:, :, None] * table_own, axis=1)
    expert_mix = jnp.dot(
        weight_table,
        returned_rows.reshape(-1, width).astype(jnp.float32),
        precision=lax.Precision.HIGHEST,
    )
    out_own = (after_own.astype(jnp.float32) + expert_mix).astype(jnp.bfloat16)
    copies = jnp.broadcast_to(out_own[None], (tp_count, *out_own.shape))
    return lax.all_to_all(copies, TP, 0, 0, tiled=True).reshape(tok_count, width)


def solution(mesh):
    torus = Mesh(mesh.devices.reshape(-1, 2, 4, mesh.shape["tp"] // 4), ALL)
    return jax.shard_map(
        shards,
        mesh=torus,
        in_specs=(
            P(SP, None),
            P(),
            P(None, TP),
            P(TP),
            P(),
            P(SP, None),
            P(SP, None),
            P(SP, None, TP),
            P(SP, None, TP),
            P(SP, TP, None),
        ),
        out_specs=P(SP, None),
        check_vma=False,
    )
```

```python
import functools
import math

import jax
import jax.numpy as jnp
import numpy as np
from jax import lax
from jax.experimental import pallas as pl
from jax.experimental.pallas import tpu as pltpu
from jax.sharding import Mesh
from jax.sharding import PartitionSpec as P

GROUPS = 4
SPAN = 16
TOP_K = 2
ROWS = 16
CAP = 2
SP = ("z", "c")
TP = ("y", "x")
ALL = ("z", "c", "y", "x")

EPS = 1e-06
LANES = 128


def from_behind(value, axis, steps):
    count = lax.axis_size(axis)
    first, last = (max(0, -steps), min(count, count - steps))
    return lax.ppermute(value, axis, [(source, source + steps) for source in range(first, last)])


def plane_groups(swapped):
    sizes = [lax.axis_size(a) for a in ALL]
    index = np.arange(math.prod(sizes)).reshape(sizes)
    groups = []
    for z in range(sizes[0]):
        for c in range(sizes[1]):
            plane = index[z, c]
            groups += (plane if (c % 2 == 0) != swapped else plane.T).tolist()
    return groups


def exchange(blocks, groups):
    return lax.all_to_all(blocks, ALL, 0, 0, tiled=True, axis_index_groups=groups)


def gather_stage(block, groups):
    return exchange(jnp.broadcast_to(block[None], (len(groups[0]), *block.shape)), groups)


def sum_stage(blocks, groups):
    return jnp.sum(exchange(blocks, groups).astype(jnp.float32), axis=0).astype(jnp.bfloat16)


def expert_kernel(side, core_ref, x_ref, gain_ref, gate_ref, up_ref, down_ref, out_ref, normed):
    count, rows, lanes = x_ref.shape
    swapped = core_ref[0]

    def place(t):
        return jnp.where(swapped == 0, t, (t % side) * side + t // side)

    squares = jnp.zeros((rows, lanes), jnp.float32)
    for t in range(count):
        values = x_ref[t].astype(jnp.float32)
        squares = squares + values * values
    inverse = lax.rsqrt(jnp.sum(squares, axis=1, keepdims=True) / (count * lanes) + EPS)
    for t in range(count):
        columns = slice(t * lanes, (t + 1) * lanes)
        values = x_ref[place(t)].astype(jnp.float32)
        normed[:, columns] = (values * inverse * gain_ref[:, columns]).astype(jnp.bfloat16)
    contract = (((1,), (1,)), ((), ()))
    gate = lax.dot_general(normed[...], gate_ref[...], contract, preferred_element_type=jnp.float32)
    up = lax.dot_general(normed[...], up_ref[...], contract, preferred_element_type=jnp.float32)
    hidden = (gate * (1.0 / (1.0 + jnp.exp(-gate))) * up).astype(jnp.bfloat16)
    for t in range(0, count, 2):
        pair = jnp.dot(
            hidden,
            down_ref[:, t * lanes : (t + 2) * lanes],
            preferred_element_type=jnp.float32,
        ).astype(jnp.bfloat16)
        out_ref[place(t)] = pair[:, :lanes]
        out_ref[place(t + 1)] = pair[:, lanes:]


def expert(blocks, core, gain, gate_t, up_t, down, side, rows=256):
    count, total, lanes = blocks.shape
    units, width = gate_t.shape
    whole = lambda shape: pl.BlockSpec(shape, lambda i, core: (0, 0))
    part = pl.BlockSpec((count, rows, lanes), lambda i, core: (0, i, 0))
    return pl.pallas_call(
        functools.partial(expert_kernel, side),
        out_shape=jax.ShapeDtypeStruct(blocks.shape, jnp.bfloat16),
        grid_spec=pltpu.PrefetchScalarGridSpec(
            num_scalar_prefetch=1,
            grid=(total // rows,),
            in_specs=[
                part,
                whole((1, width)),
                whole((units, width)),
                whole((units, width)),
                whole((units, width)),
            ],
            out_specs=part,
            scratch_shapes=[pltpu.VMEM((rows, width), jnp.bfloat16)],
        ),
        compiler_params=pltpu.CompilerParams(
            dimension_semantics=("arbitrary",), vmem_limit_bytes=32 * 2**20
        ),
        cost_estimate=pl.CostEstimate(
            flops=6 * total * units * width,
            bytes_accessed=4 * total * width + 6 * units * width,
            transcendentals=total * units,
        ),
        name="expert",
    )(core, blocks, gain[None], gate_t, up_t, down)


def shards(
    residual_in,
    mix_gain,
    pool_weight,
    pool_scale,
    ffn_gain,
    route_ids,
    route_weights,
    gate_weight,
    up_weight,
    down_weight,
):
    tp_count = lax.axis_size(TP)
    sp_count = lax.axis_size(SP)
    tp_index = lax.axis_index(TP)
    sp_index = lax.axis_index(SP)
    tok_count, width = residual_in.shape
    group_width = width // GROUPS
    col_count = pool_weight.shape[1]
    slots = tok_count // ROWS * CAP
    group_index = tp_index * col_count // group_width

    rim = from_behind(residual_in[tok_count - SPAN :], SP, 1)

    def normed_group(rows):
        rows = rows.astype(jnp.float32)
        inverse = lax.rsqrt(jnp.mean(rows * rows, axis=-1, keepdims=True) + EPS)
        part = lax.dynamic_slice_in_dim(rows, group_index * group_width, group_width, 1)
        gain = lax.dynamic_slice_in_dim(mix_gain, group_index * group_width, group_width, 0)
        return (part * inverse * gain).astype(jnp.bfloat16).astype(jnp.float32)

    extended = jnp.concatenate([normed_group(rim), normed_group(residual_in)], axis=0)
    window_sum, sums = (None, extended)
    for step in range(GROUPS):
        reach = 2**step
        sums = sums[reach:] + sums[:-reach]
        here = sums[sums.shape[0] - tok_count :]
        window_sum = here if step == 0 else jnp.where(group_index == step, here, window_sum)
    window = jnp.left_shift(2, group_index)
    position = sp_index * tok_count + jnp.arange(tok_count, dtype=jnp.int32)
    divisor = jnp.minimum(position + 1, window).astype(jnp.float32)
    pooled = (window_sum / divisor[:, None] - extended[SPAN:]).astype(jnp.bfloat16)
    mixed = (jnp.dot(pooled, pool_weight, preferred_element_type=jnp.float32) * pool_scale).astype(
        jnp.bfloat16
    )
    stream = lax.dynamic_slice_in_dim(residual_in, tp_index * col_count, col_count, 1)
    after = (stream.astype(jnp.float32) + mixed.astype(jnp.float32)).astype(jnp.bfloat16)

    token = np.arange(tok_count)
    earlier = (token[:, None] // ROWS == token[None, :] // ROWS) & (token[None, :] < token[:, None])
    experts = jnp.arange(sp_count, dtype=jnp.int32)
    named = [(route_ids[:, k : k + 1] == experts[None, :]).astype(jnp.float32) for k in range(TOP_K)]
    before = jnp.dot(
        jnp.asarray(earlier, jnp.bfloat16),
        sum(named).astype(jnp.bfloat16),
        preferred_element_type=jnp.float32,
    )
    slot = jnp.arange(sp_count * slots, dtype=jnp.int32)
    block = jnp.asarray(token // ROWS * CAP, jnp.int32)
    tables = []
    for k in range(TOP_K):
        slot_of = jnp.sum(before * named[k], axis=1).astype(jnp.int32)
        target = route_ids[:, k] * slots + block + slot_of
        tables.append(target[:, None] == slot[None, :])
    outgoing = lax.dot_general(
        (tables[0] | tables[1]).astype(jnp.bfloat16),
        after,
        (((0,), (0,)), ((), ())),
        preferred_element_type=jnp.float32,
    ).astype(jnp.bfloat16)
    arrived = lax.all_to_all(outgoing.reshape(sp_count, slots, col_count), SP, 0, 0, tiled=True)
    arrived = arrived.reshape(sp_count * slots, col_count)

    first, second = (plane_groups(False), plane_groups(True))
    side = len(first[0])
    gathered = gather_stage(gather_stage(arrived, first), second)
    core = lax.axis_index("c").astype(jnp.int32).reshape(1)
    term = expert(
        gathered.reshape(tp_count, *arrived.shape),
        core,
        ffn_gain,
        gate_weight[0].T,
        up_weight[0].T,
        down_weight[0],
        side,
    )
    expert_out = sum_stage(sum_stage(term.reshape(side, side, *arrived.shape), second), first)
    returned = lax.all_to_all(
        expert_out.reshape(sp_count, slots, col_count), SP, 0, 0, tiled=True
    ).reshape(sp_count * slots, col_count)
    weights = sum(
        jnp.where(tables[k], route_weights[:, k : k + 1], 0.0) for k in range(TOP_K)
    )
    expert_mix = jnp.dot(
        weights, returned.astype(jnp.float32), precision=lax.Precision.HIGHEST
    )
    out = (after.astype(jnp.float32) + expert_mix).astype(jnp.bfloat16)
    copies = jnp.broadcast_to(out[None], (tp_count, *out.shape))
    columns = lax.all_to_all(copies, TP, 0, 0, tiled=True)
    return jnp.concatenate([columns[t] for t in range(tp_count)], axis=1)


def solution(mesh):
    torus = Mesh(mesh.devices.reshape(-1, 2, 4, mesh.shape["tp"] // 4), ALL)
    return jax.shard_map(
        shards,
        mesh=torus,
        in_specs=(
            P(SP, None),
            P(),
            P(None, TP),
            P(TP),
            P(),
            P(SP, None),
            P(SP, None),
            P(SP, None, TP),
            P(SP, None, TP),
            P(SP, TP, None),
        ),
        out_specs=P(SP, None),
        check_vma=False,
    )
```

```python
import functools
import math

import jax
import jax.numpy as jnp
import numpy as np
from jax import lax
from jax.experimental import pallas as pl
from jax.experimental.pallas import tpu as pltpu
from jax.sharding import Mesh
from jax.sharding import PartitionSpec as P

GROUPS = 4
SPAN = 16
TOP_K = 2
ROWS = 16
CAP = 2
SP = ("z", "c")
TP = ("y", "x")
ALL = ("z", "c", "y", "x")

EPS = 1e-06
LANES = 128


def from_behind(value, axis, steps):
    count = lax.axis_size(axis)
    first, last = (max(0, -steps), min(count, count - steps))
    return lax.ppermute(value, axis, [(source, source + steps) for source in range(first, last)])


def planes():
    sizes = [lax.axis_size(a) for a in ALL]
    index = np.arange(math.prod(sizes)).reshape(sizes)
    return [
        index[z, c] if c % 2 == 0 else index[z, c].T
        for z in range(sizes[0])
        for c in range(sizes[1])
    ]


def from_quad(value, steps):
    pairs = []
    for plane in planes():
        pairs += list(zip(plane.ravel().tolist(), np.roll(plane, -steps, axis=1).ravel().tolist()))
    return lax.ppermute(value, ALL, pairs)


def exchange(blocks):
    groups = [plane.ravel().tolist() for plane in planes()]
    return lax.all_to_all(blocks, ALL, 0, 0, tiled=True, axis_index_groups=groups)


def place(t, side, swapped):
    return jnp.where(swapped == 0, t, (t % side) * side + t // side)


def norm_kernel(side, core_ref, x_ref, gain_ref, normed_ref):
    count, rows, lanes = x_ref.shape
    squares = jnp.zeros((rows, lanes), jnp.float32)
    for t in range(count):
        values = x_ref[t].astype(jnp.float32)
        squares = squares + values * values
    inverse = lax.rsqrt(jnp.sum(squares, axis=1, keepdims=True) / (count * lanes) + EPS)
    for t in range(count):
        columns = slice(t * lanes, (t + 1) * lanes)
        values = x_ref[place(t, side, core_ref[0])].astype(jnp.float32)
        normed_ref[:, columns] = (values * inverse * gain_ref[:, columns]).astype(jnp.bfloat16)


def expert_kernel(side, parts, core_ref, normed_ref, *refs):
    weight_refs, refs = (refs[:parts], refs[parts:])
    last = len(refs[-1].shape) == 3
    total_refs, out_ref = (refs[:-1], refs[-1])
    width = normed_ref.shape[1]
    units = weight_refs[0].shape[0] // 3
    contract = (((1,), (1,)), ((), ()))
    normed = normed_ref[...]
    hidden = []
    for ref in weight_refs:
        gate = lax.dot_general(normed, ref[:units], contract, preferred_element_type=jnp.float32)
        up = lax.dot_general(
            normed, ref[units : 2 * units], contract, preferred_element_type=jnp.float32
        )
        hidden.append((gate * (1.0 / (1.0 + jnp.exp(-gate))) * up).astype(jnp.bfloat16))
    step = 2 * LANES
    for first in range(0, width, step):
        columns = slice(first, first + step)
        total = 0.0
        for part, ref in zip(hidden, weight_refs):
            total = total + jnp.dot(
                part, ref[2 * units :, columns], preferred_element_type=jnp.float32
            )
        for ref in total_refs:
            total = total + ref[:, columns]
        if last:
            for half in range(2):
                t = first // LANES + half
                out_ref[place(t, side, core_ref[0])] = total[
                    :, half * LANES : (half + 1) * LANES
                ].astype(jnp.bfloat16)
        else:
            out_ref[:, columns] = total


SCALARS = pl.BlockSpec(memory_space=pltpu.SMEM)
VECTORS = pl.BlockSpec(memory_space=pltpu.VMEM)


def norm_rows(blocks, core, gain, side):
    count, rows, lanes = blocks.shape
    return pl.pallas_call(
        functools.partial(norm_kernel, side),
        out_shape=jax.ShapeDtypeStruct((rows, count * lanes), jnp.bfloat16),
        in_specs=[SCALARS, VECTORS, VECTORS],
        out_specs=VECTORS,
        cost_estimate=pl.CostEstimate(
            flops=4 * blocks.size, bytes_accessed=4 * blocks.size, transcendentals=rows
        ),
        name="norm",
    )(core, blocks, gain[None])


def expert(normed, core, weights, totals, side, last):
    rows, width = normed.shape
    units = weights[0].shape[0] // 3
    if last:
        out = jax.ShapeDtypeStruct((width // LANES, rows, LANES), jnp.bfloat16)
    else:
        out = jax.ShapeDtypeStruct((rows, width), jnp.float32)
    return pl.pallas_call(
        functools.partial(expert_kernel, side, len(weights)),
        out_shape=out,
        in_specs=[SCALARS] + [VECTORS] * (1 + len(weights) + len(totals)),
        out_specs=VECTORS,
        compiler_params=pltpu.CompilerParams(vmem_limit_bytes=40 * 2**20),
        cost_estimate=pl.CostEstimate(
            flops=6 * rows * units * width * len(weights),
            bytes_accessed=6 * units * width * len(weights),
            transcendentals=rows * units * len(weights),
        ),
        name="expert",
    )(core, normed, *weights, *totals)


def assemble_kernel(columns_ref, out_ref):
    for t in range(columns_ref.shape[0]):
        out_ref[:, t * LANES : (t + 1) * LANES] = columns_ref[t]


def assemble(columns, rows=64):
    count, total, lanes = columns.shape
    return pl.pallas_call(
        assemble_kernel,
        out_shape=jax.ShapeDtypeStruct((total, count * lanes), columns.dtype),
        grid=(total // rows,),
        in_specs=[pl.BlockSpec((count, rows, lanes), lambda i: (0, i, 0))],
        out_specs=pl.BlockSpec((rows, count * lanes), lambda i: (i, 0)),
        name="assemble",
    )(columns)


def shards(
    residual_in,
    mix_gain,
    pool_weight,
    pool_scale,
    ffn_gain,
    route_ids,
    route_weights,
    gate_weight,
    up_weight,
    down_weight,
):
    tp_count = lax.axis_size(TP)
    sp_count = lax.axis_size(SP)
    tp_index = lax.axis_index(TP)
    sp_index = lax.axis_index(SP)
    tok_count, width = residual_in.shape
    group_width = width // GROUPS
    col_count = pool_weight.shape[1]
    slots = tok_count // ROWS * CAP
    group_index = tp_index * col_count // group_width

    own = jnp.concatenate([gate_weight[0].T, up_weight[0].T, down_weight[0]], axis=0)
    others = [from_quad(own, steps) for steps in (1, -1, 2)]
    rim = from_behind(residual_in[tok_count - SPAN :], SP, 1)

    def normed_group(rows):
        rows = rows.astype(jnp.float32)
        inverse = lax.rsqrt(jnp.mean(rows * rows, axis=-1, keepdims=True) + EPS)
        part = lax.dynamic_slice_in_dim(rows, group_index * group_width, group_width, 1)
        gain = lax.dynamic_slice_in_dim(mix_gain, group_index * group_width, group_width, 0)
        return lax.reduce_precision(part * inverse * gain, 8, 7)

    extended = jnp.concatenate([normed_group(rim), normed_group(residual_in)], axis=0)
    window_sum, sums = (None, extended)
    for step in range(GROUPS):
        reach = 2**step
        sums = sums[reach:] + sums[:-reach]
        here = sums[sums.shape[0] - tok_count :]
        window_sum = here if step == 0 else jnp.where(group_index == step, here, window_sum)
    window = jnp.left_shift(2, group_index)
    position = sp_index * tok_count + jnp.arange(tok_count, dtype=jnp.int32)
    divisor = jnp.minimum(position + 1, window).astype(jnp.float32)
    pooled = (window_sum / divisor[:, None] - extended[SPAN:]).astype(jnp.bfloat16)
    mixed = (jnp.dot(pooled, pool_weight, preferred_element_type=jnp.float32) * pool_scale).astype(
        jnp.bfloat16
    )
    stream = lax.dynamic_slice_in_dim(residual_in, tp_index * col_count, col_count, 1)
    after = (stream.astype(jnp.float32) + mixed.astype(jnp.float32)).astype(jnp.bfloat16)

    token = np.arange(tok_count)
    earlier = (token[:, None] // ROWS == token[None, :] // ROWS) & (token[None, :] < token[:, None])
    experts = jnp.arange(sp_count, dtype=jnp.int32)
    named = [(route_ids[:, k : k + 1] == experts[None, :]).astype(jnp.float32) for k in range(TOP_K)]
    before = jnp.dot(
        jnp.asarray(earlier, jnp.bfloat16),
        sum(named).astype(jnp.bfloat16),
        preferred_element_type=jnp.float32,
    )
    slot = jnp.arange(sp_count * slots, dtype=jnp.int32)
    block = jnp.asarray(token // ROWS * CAP, jnp.int32)
    tables = []
    for k in range(TOP_K):
        slot_of = jnp.sum(before * named[k], axis=1).astype(jnp.int32)
        target = route_ids[:, k] * slots + block + slot_of
        tables.append(target[:, None] == slot[None, :])
    outgoing = lax.dot_general(
        (tables[0] | tables[1]).astype(jnp.bfloat16),
        after,
        (((0,), (0,)), ((), ())),
        preferred_element_type=jnp.float32,
    ).astype(jnp.bfloat16)
    arrived = lax.all_to_all(outgoing.reshape(sp_count, slots, col_count), SP, 0, 0, tiled=True)
    arrived = arrived.reshape(sp_count * slots, col_count)

    side = lax.axis_size("x")
    core = lax.axis_index("c").astype(jnp.int32).reshape(1)
    quarter = arrived.reshape(1, side, -1, col_count)
    quarter = jnp.broadcast_to(quarter, (side, *quarter.shape[1:]))
    gathered = exchange(quarter.reshape(tp_count, -1, col_count))
    normed = norm_rows(gathered, core, ffn_gain, side)
    total = expert(normed, core, [own, *others[:2]], [], side, False)
    term = expert(normed, core, others[2:], [total], side, True)
    summed = exchange(term).reshape(quarter.shape)
    expert_out = jnp.sum(summed.astype(jnp.float32), axis=0).astype(jnp.bfloat16)
    returned = lax.all_to_all(
        expert_out.reshape(sp_count, slots, col_count), SP, 0, 0, tiled=True
    ).reshape(sp_count * slots, col_count)
    weights = sum(
        jnp.where(tables[k], route_weights[:, k : k + 1], 0.0) for k in range(TOP_K)
    )
    expert_mix = jnp.dot(
        weights, returned.astype(jnp.float32), precision=lax.Precision.HIGHEST
    )
    out = (after.astype(jnp.float32) + expert_mix).astype(jnp.bfloat16)
    copies = jnp.broadcast_to(out[None], (tp_count, *out.shape))
    columns = lax.all_to_all(copies, TP, 0, 0, tiled=True)
    return assemble(columns)


def solution(mesh):
    torus = Mesh(mesh.devices.reshape(-1, 2, 4, mesh.shape["tp"] // 4), ALL)
    return jax.shard_map(
        shards,
        mesh=torus,
        in_specs=(
            P(SP, None),
            P(),
            P(None, TP),
            P(TP),
            P(),
            P(SP, None),
            P(SP, None),
            P(SP, None, TP),
            P(SP, None, TP),
            P(SP, TP, None),
        ),
        out_specs=P(SP, None),
        check_vma=False,
    )
```

```python
import functools
import math

import jax
import jax.numpy as jnp
import numpy as np
from jax import lax
from jax.experimental import pallas as pl
from jax.experimental.pallas import tpu as pltpu
from jax.sharding import Mesh
from jax.sharding import PartitionSpec as P

GROUPS = 4
SPAN = 16
TOP_K = 2
ROWS = 16
CAP = 2
SP = ("z", "c")
TP = ("y", "x")
ALL = ("z", "c", "y", "x")

EPS = 1e-06
LANES = 128


def from_behind(value, axis, steps):
    count = lax.axis_size(axis)
    first, last = (max(0, -steps), min(count, count - steps))
    return lax.ppermute(value, axis, [(source, source + steps) for source in range(first, last)])


def planes():
    sizes = [lax.axis_size(a) for a in ALL]
    index = np.arange(math.prod(sizes)).reshape(sizes)
    return [
        index[z, c] if c % 2 == 0 else index[z, c].T
        for z in range(sizes[0])
        for c in range(sizes[1])
    ]


def from_quad(value, steps):
    pairs = []
    for plane in planes():
        pairs += list(zip(plane.ravel().tolist(), np.roll(plane, -steps, axis=1).ravel().tolist()))
    return lax.ppermute(value, ALL, pairs)


def exchange(blocks):
    groups = [plane.ravel().tolist() for plane in planes()]
    return lax.all_to_all(blocks, ALL, 0, 0, tiled=True, axis_index_groups=groups)


def place(t, side, swapped):
    return jnp.where(swapped == 0, t, (t % side) * side + t // side)


def expert_kernel(side, core_ref, x_ref, gain_ref, *refs):
    pieces = (len(refs) - 3) // 2
    sources, out_ref, normed_ref = (refs[:pieces], refs[pieces], refs[pieces + 1])
    weights, semaphores = (refs[pieces + 2 : 2 * pieces + 2], refs[-1])
    copies = [
        pltpu.make_async_copy(source, target, semaphores.at[i])
        for i, (source, target) in enumerate(zip(sources, weights))
    ]
    for copy in copies:
        copy.start()
    count, rows, lanes = x_ref.shape
    squares = jnp.zeros((rows, lanes), jnp.float32)
    for t in range(count):
        values = x_ref[t].astype(jnp.float32)
        squares = squares + values * values
    inverse = lax.rsqrt(jnp.sum(squares, axis=1, keepdims=True) / (count * lanes) + EPS)
    for t in range(count):
        columns = slice(t * lanes, (t + 1) * lanes)
        values = x_ref[place(t, side, core_ref[0])].astype(jnp.float32)
        normed_ref[:, columns] = (values * inverse * gain_ref[:, columns]).astype(jnp.bfloat16)
    units = weights[0].shape[0] // 3
    contract = (((1,), (1,)), ((), ()))
    normed = normed_ref[...]
    hidden, downs = ([], [])
    for i in range(pieces - 1):
        copies[i].wait()
        gate_rows, up_rows = (weights[i][:units], None)
        if i < pieces - 2:
            up_rows = weights[i][units : 2 * units]
            downs.append(weights[i].at[2 * units :])
        else:
            copies[i + 1].wait()
            cut = weights[i].shape[0]
            up_rows = jnp.concatenate(
                [weights[i][units:], weights[i + 1][: 2 * units - cut]], axis=0
            )
            downs.append(weights[i + 1].at[2 * units - cut :])
        gate = lax.dot_general(normed, gate_rows, contract, preferred_element_type=jnp.float32)
        up = lax.dot_general(normed, up_rows, contract, preferred_element_type=jnp.float32)
        hidden.append((gate * (1.0 / (1.0 + jnp.exp(-gate))) * up).astype(jnp.bfloat16))
    for t in range(0, count, 2):
        total = 0.0
        for part, down in zip(hidden, downs):
            total = total + jnp.dot(
                part,
                down[:, t * lanes : (t + 2) * lanes],
                preferred_element_type=jnp.float32,
            )
        total = total.astype(jnp.bfloat16)
        out_ref[place(t, side, core_ref[0])] = total[:, :lanes]
        out_ref[place(t + 1, side, core_ref[0])] = total[:, lanes:]


SCALARS = pl.BlockSpec(memory_space=pltpu.SMEM)
VECTORS = pl.BlockSpec(memory_space=pltpu.VMEM)
ANYWHERE = pl.BlockSpec(memory_space=pl.ANY)


def expert(blocks, core, gain, weights, side):
    count, rows, lanes = blocks.shape
    width = count * lanes
    units = weights[0].shape[0] // 3
    return pl.pallas_call(
        functools.partial(expert_kernel, side),
        out_shape=jax.ShapeDtypeStruct(blocks.shape, jnp.bfloat16),
        in_specs=[SCALARS, VECTORS, VECTORS] + [ANYWHERE] * len(weights),
        out_specs=VECTORS,
        scratch_shapes=[pltpu.VMEM((rows, width), jnp.bfloat16)]
        + [pltpu.VMEM(w.shape, w.dtype) for w in weights]
        + [pltpu.SemaphoreType.DMA((len(weights),))],
        compiler_params=pltpu.CompilerParams(vmem_limit_bytes=32 * 2**20),
        cost_estimate=pl.CostEstimate(
            flops=6 * rows * units * width * side,
            bytes_accessed=6 * units * width * side,
            transcendentals=rows * units * side,
        ),
        name="expert",
    )(core, blocks, gain[None], *weights)


def assemble_kernel(columns_ref, out_ref):
    rows = out_ref.shape[0]
    here = pl.ds(pl.multiple_of(pl.program_id(0) * rows, rows), rows)
    for t in range(columns_ref.shape[0]):
        out_ref[:, t * LANES : (t + 1) * LANES] = columns_ref[t, here]


def assemble(columns, rows=64):
    count, total, lanes = columns.shape
    return pl.pallas_call(
        assemble_kernel,
        out_shape=jax.ShapeDtypeStruct((total, count * lanes), columns.dtype),
        grid=(total // rows,),
        in_specs=[VECTORS],
        out_specs=pl.BlockSpec((rows, count * lanes), lambda i: (i, 0)),
        name="assemble",
    )(columns)


def layer(
    residual_in,
    mix_gain,
    pool_weight,
    pool_scale,
    ffn_gain,
    route_ids,
    route_weights,
    gate_weight,
    up_weight,
    down_weight,
):
    tp_count = lax.axis_size(TP)
    sp_count = lax.axis_size(SP)
    tp_index = lax.axis_index(TP)
    sp_index = lax.axis_index(SP)
    tok_count, width = residual_in.shape
    group_width = width // GROUPS
    col_count = pool_weight.shape[1]
    slots = tok_count // ROWS * CAP
    group_index = tp_index * col_count // group_width

    own = jnp.concatenate([gate_weight[0].T, up_weight[0].T, down_weight[0]], axis=0)
    left = from_quad(own, 1)
    right = from_quad(own, -1)
    rim = from_behind(residual_in[tok_count - SPAN :], SP, 1)

    def normed_group(rows):
        rows = rows.astype(jnp.float32)
        inverse = lax.rsqrt(jnp.mean(rows * rows, axis=-1, keepdims=True) + EPS)
        part = lax.dynamic_slice_in_dim(rows, group_index * group_width, group_width, 1)
        gain = lax.dynamic_slice_in_dim(mix_gain, group_index * group_width, group_width, 0)
        return lax.reduce_precision(part * inverse * gain, 8, 7)

    extended = jnp.concatenate([normed_group(rim), normed_group(residual_in)], axis=0)
    window_sum, sums = (None, extended)
    for step in range(GROUPS):
        reach = 2**step
        sums = sums[reach:] + sums[:-reach]
        here = sums[sums.shape[0] - tok_count :]
        window_sum = here if step == 0 else jnp.where(group_index == step, here, window_sum)
    window = jnp.left_shift(2, group_index)
    position = sp_index * tok_count + jnp.arange(tok_count, dtype=jnp.int32)
    divisor = jnp.minimum(position + 1, window).astype(jnp.float32)
    pooled = (window_sum / divisor[:, None] - extended[SPAN:]).astype(jnp.bfloat16)
    mixed = (jnp.dot(pooled, pool_weight, preferred_element_type=jnp.float32) * pool_scale).astype(
        jnp.bfloat16
    )
    stream = lax.dynamic_slice_in_dim(residual_in, tp_index * col_count, col_count, 1)
    after = (stream.astype(jnp.float32) + mixed.astype(jnp.float32)).astype(jnp.bfloat16)

    token = np.arange(tok_count)
    earlier = (token[:, None] // ROWS == token[None, :] // ROWS) & (token[None, :] < token[:, None])
    experts = jnp.arange(sp_count, dtype=jnp.int32)
    named = [(route_ids[:, k : k + 1] == experts[None, :]).astype(jnp.float32) for k in range(TOP_K)]
    before = jnp.dot(
        jnp.asarray(earlier, jnp.bfloat16),
        sum(named).astype(jnp.bfloat16),
        preferred_element_type=jnp.float32,
    )
    slot = jnp.arange(sp_count * slots, dtype=jnp.int32)
    block = jnp.asarray(token // ROWS * CAP, jnp.int32)
    tables = []
    for k in range(TOP_K):
        slot_of = jnp.sum(before * named[k], axis=1).astype(jnp.int32)
        target = route_ids[:, k] * slots + block + slot_of
        tables.append(target[:, None] == slot[None, :])
    outgoing = lax.dot_general(
        (tables[0] | tables[1]).astype(jnp.bfloat16),
        after,
        (((0,), (0,)), ((), ())),
        preferred_element_type=jnp.float32,
    ).astype(jnp.bfloat16)
    outgoing = outgoing.reshape(sp_count, slots, col_count)
    arrived = lax.all_to_all(outgoing, SP, 0, 0, tiled=True)
    half = own.shape[0] // 2
    upper = left[:half]
    lower = right[half:]
    upper = from_quad(upper, 1)
    lower = from_quad(lower, -1)
    arrived = arrived.reshape(sp_count * slots, col_count)

    side = lax.axis_size("x")
    core = lax.axis_index("c").astype(jnp.int32).reshape(1)
    quarter = arrived.reshape(1, side, -1, col_count)
    quarter = jnp.broadcast_to(quarter, (side, *quarter.shape[1:]))
    gathered = exchange(quarter.reshape(tp_count, -1, col_count))
    term = expert(gathered, core, ffn_gain, [own, left, right, upper, lower], side)
    summed = exchange(term).reshape(quarter.shape)
    expert_out = jnp.sum(summed.astype(jnp.float32), axis=0).astype(jnp.bfloat16)
    returned = lax.all_to_all(
        expert_out.reshape(sp_count, slots, col_count), SP, 0, 0, tiled=True
    ).reshape(sp_count * slots, col_count)
    weights = sum(
        jnp.where(tables[k], route_weights[:, k : k + 1], 0.0) for k in range(TOP_K)
    )
    expert_mix = jnp.dot(
        weights, returned.astype(jnp.float32), precision=lax.Precision.HIGHEST
    )
    out = (after.astype(jnp.float32) + expert_mix).astype(jnp.bfloat16)
    copies = jnp.broadcast_to(out[None], (tp_count, *out.shape))
    columns = lax.all_to_all(copies, TP, 0, 0, tiled=True)
    return assemble(columns)


def solution(mesh):
    torus = Mesh(mesh.devices.reshape(-1, 2, 4, mesh.shape["tp"] // 4), ALL)
    return jax.shard_map(
        layer,
        mesh=torus,
        in_specs=(
            P(SP, None),
            P(),
            P(None, TP),
            P(TP),
            P(),
            P(SP, None),
            P(SP, None),
            P(SP, None, TP),
            P(SP, None, TP),
            P(SP, TP, None),
        ),
        out_specs=P(SP, None),
        check_vma=False,
    )
```

```python
import functools
import math

import jax
import jax.numpy as jnp
import numpy as np
from jax import lax
from jax.experimental import pallas as pl
from jax.experimental.pallas import tpu as pltpu
from jax.sharding import Mesh
from jax.sharding import PartitionSpec as P

GROUPS = 4
SPAN = 16
TOP_K = 2
ROWS = 16
CAP = 2
SP = ("z", "c")
TP = ("y", "x")
ALL = ("z", "c", "y", "x")

EPS = 1e-06
LANES = 128


def from_behind(value, axis, steps):
    count = lax.axis_size(axis)
    first, last = (max(0, -steps), min(count, count - steps))
    return lax.ppermute(value, axis, [(source, source + steps) for source in range(first, last)])


def planes():
    sizes = [lax.axis_size(a) for a in ALL]
    index = np.arange(math.prod(sizes)).reshape(sizes)
    return [
        index[z, c] if c % 2 == 0 else index[z, c].T
        for z in range(sizes[0])
        for c in range(sizes[1])
    ]


def from_quad(value, steps):
    pairs = []
    for plane in planes():
        pairs += list(zip(plane.ravel().tolist(), np.roll(plane, -steps, axis=1).ravel().tolist()))
    return lax.ppermute(value, ALL, pairs)


def exchange(blocks):
    groups = [plane.ravel().tolist() for plane in planes()]
    return lax.all_to_all(blocks, ALL, 0, 0, tiled=True, axis_index_groups=groups)


def place(t, side, swapped):
    return jnp.where(swapped == 0, t, (t % side) * side + t // side)


def expert_kernel(side, core_ref, x_ref, gain_ref, *refs):
    pieces = (len(refs) - 3) // 2
    sources, out_ref, normed_ref = (refs[:pieces], refs[pieces], refs[pieces + 1])
    weights, semaphores = (refs[pieces + 2 : 2 * pieces + 2], refs[-1])
    copies = [
        pltpu.make_async_copy(source, target, semaphores.at[i])
        for i, (source, target) in enumerate(zip(sources, weights))
    ]
    for copy in copies:
        copy.start()
    count, rows, lanes = x_ref.shape
    squares = jnp.zeros((rows, lanes), jnp.float32)
    for t in range(count):
        values = x_ref[t].astype(jnp.float32)
        squares = squares + values * values
    inverse = lax.rsqrt(jnp.sum(squares, axis=1, keepdims=True) / (count * lanes) + EPS)
    for t in range(count):
        columns = slice(t * lanes, (t + 1) * lanes)
        values = x_ref[place(t, side, core_ref[0])].astype(jnp.float32)
        normed_ref[:, columns] = (values * inverse * gain_ref[:, columns]).astype(jnp.bfloat16)
    units = weights[0].shape[0] // 3
    contract = (((1,), (1,)), ((), ()))
    normed = normed_ref[...]
    hidden, downs = ([], [])
    for i in range(pieces - 1):
        copies[i].wait()
        gate_rows, up_rows = (weights[i][:units], None)
        if i < pieces - 2:
            up_rows = weights[i][units : 2 * units]
            downs.append(weights[i].at[2 * units :])
        else:
            copies[i + 1].wait()
            cut = weights[i].shape[0]
            up_rows = jnp.concatenate(
                [weights[i][units:], weights[i + 1][: 2 * units - cut]], axis=0
            )
            downs.append(weights[i + 1].at[2 * units - cut :])
        gate = lax.dot_general(normed, gate_rows, contract, preferred_element_type=jnp.float32)
        up = lax.dot_general(normed, up_rows, contract, preferred_element_type=jnp.float32)
        hidden.append((gate * (1.0 / (1.0 + jnp.exp(-gate))) * up).astype(jnp.bfloat16))
    for t in range(0, count, 2):
        total = 0.0
        for part, down in zip(hidden, downs):
            total = total + jnp.dot(
                part,
                down[:, t * lanes : (t + 2) * lanes],
                preferred_element_type=jnp.float32,
            )
        total = total.astype(jnp.bfloat16)
        out_ref[place(t, side, core_ref[0])] = total[:, :lanes]
        out_ref[place(t + 1, side, core_ref[0])] = total[:, lanes:]


SCALARS = pl.BlockSpec(memory_space=pltpu.SMEM)
VECTORS = pl.BlockSpec(memory_space=pltpu.VMEM)
ANYWHERE = pl.BlockSpec(memory_space=pl.ANY)


def expert(blocks, core, gain, weights, side):
    count, rows, lanes = blocks.shape
    width = count * lanes
    units = weights[0].shape[0] // 3
    return pl.pallas_call(
        functools.partial(expert_kernel, side),
        out_shape=jax.ShapeDtypeStruct(blocks.shape, jnp.bfloat16),
        in_specs=[SCALARS, VECTORS, VECTORS] + [ANYWHERE] * len(weights),
        out_specs=VECTORS,
        scratch_shapes=[pltpu.VMEM((rows, width), jnp.bfloat16)]
        + [pltpu.VMEM(w.shape, w.dtype) for w in weights]
        + [pltpu.SemaphoreType.DMA((len(weights),))],
        compiler_params=pltpu.CompilerParams(vmem_limit_bytes=32 * 2**20),
        cost_estimate=pl.CostEstimate(
            flops=6 * rows * units * width * side,
            bytes_accessed=6 * units * width * side,
            transcendentals=rows * units * side,
        ),
        name="expert",
    )(core, blocks, gain[None], *weights)


def inverse_rms(ref):
    rows, width = ref.shape
    squares = jnp.zeros((rows, LANES), jnp.float32)
    for first in range(0, width, LANES):
        values = ref[:, first : first + LANES].astype(jnp.float32)
        squares = squares + values * values
    return lax.rsqrt(jnp.sum(squares, axis=1, keepdims=True) / width + EPS)


def mixer_kernel(
    experts,
    index_ref,
    ids_ref,
    x_ref,
    rim_ref,
    gain_ref,
    weight_ref,
    scale_ref,
    outgoing_ref,
    after_ref,
    target_ref,
):
    group, tp_index, sp_index = (index_ref[0], index_ref[1], index_ref[2])
    rows = x_ref.shape[0]
    span = rim_ref.shape[0]
    group_width, col_count = weight_ref.shape
    columns = pl.ds(pl.multiple_of(group * group_width, group_width), group_width)
    gain = gain_ref[:, columns]

    def normed(ref):
        return (ref[:, columns].astype(jnp.float32) * inverse_rms(ref) * gain).astype(jnp.bfloat16)

    window = jnp.left_shift(2, group)
    here = normed(x_ref)
    row = lax.broadcasted_iota(jnp.int32, (rows, rows), 0)
    col = lax.broadcasted_iota(jnp.int32, (rows, rows), 1)
    band = ((col <= row) & (row - col < window)).astype(jnp.bfloat16)
    sums = jnp.dot(band, here, preferred_element_type=jnp.float32)
    behind = lax.broadcasted_iota(jnp.int32, (rows, span), 0) + span
    behind = behind - lax.broadcasted_iota(jnp.int32, (rows, span), 1)
    sums = sums + jnp.dot(
        (behind < window).astype(jnp.bfloat16), normed(rim_ref), preferred_element_type=jnp.float32
    )
    position = sp_index * rows + lax.broadcasted_iota(jnp.int32, (rows, 1), 0)
    divisor = jnp.minimum(position + 1, window).astype(jnp.float32)
    pooled = (sums / divisor - here.astype(jnp.float32)).astype(jnp.bfloat16)
    mixed = jnp.dot(pooled, weight_ref[...], preferred_element_type=jnp.float32) * scale_ref[...]
    own = pl.ds(pl.multiple_of(tp_index * col_count, col_count), col_count)
    stream = x_ref[:, own].astype(jnp.float32)
    after = (stream + mixed.astype(jnp.bfloat16).astype(jnp.float32)).astype(jnp.bfloat16)
    after_ref[...] = after

    ids = ids_ref[...]
    expert_index = lax.broadcasted_iota(jnp.int32, (experts, rows), 0)
    named = [(ids[k : k + 1] == expert_index).astype(jnp.float32) for k in range(TOP_K)]
    earlier = ((row // ROWS == col // ROWS) & (row < col)).astype(jnp.bfloat16)
    before = jnp.dot(
        sum(named).astype(jnp.bfloat16), earlier, preferred_element_type=jnp.float32
    )
    slots = rows // ROWS * CAP
    block = lax.broadcasted_iota(jnp.int32, (1, rows), 1) // ROWS * CAP
    targets = []
    for k in range(TOP_K):
        slot = jnp.sum(before * named[k], axis=0, keepdims=True).astype(jnp.int32)
        targets.append(ids[k : k + 1] * slots + block + slot)
        target_ref[k : k + 1] = targets[k]
    for first in range(0, experts * slots, rows):
        place_here = row + first
        chosen = (place_here == targets[0]) | (place_here == targets[1])
        outgoing_ref[first : first + rows] = jnp.dot(
            chosen.astype(jnp.bfloat16), after, preferred_element_type=jnp.float32
        ).astype(jnp.bfloat16)


def mixer(index, ids, x, rim, gain, weight, scale, experts):
    rows = x.shape[0]
    col_count = weight.shape[1]
    slots = rows // ROWS * CAP
    return pl.pallas_call(
        functools.partial(mixer_kernel, experts),
        out_shape=(
            jax.ShapeDtypeStruct((experts * slots, col_count), jnp.bfloat16),
            jax.ShapeDtypeStruct((rows, col_count), jnp.bfloat16),
            jax.ShapeDtypeStruct((TOP_K, rows), jnp.int32),
        ),
        in_specs=[SCALARS] + [VECTORS] * 6,
        out_specs=(VECTORS,) * 3,
        compiler_params=pltpu.CompilerParams(vmem_limit_bytes=16 * 2**20),
        cost_estimate=pl.CostEstimate(
            flops=10**9, bytes_accessed=4 * x.size, transcendentals=rows
        ),
        name="mixer",
    )(index, ids, x, rim, gain[None], weight, scale[None])


def halves_kernel(left_ref, right_ref, upper_ref, lower_ref):
    upper_ref[...] = left_ref[...]
    lower_ref[...] = right_ref[...]


def halves(left, right, steps=3):
    total, width = left.shape
    rows = total // 2 // steps
    first = pl.BlockSpec((rows, width), lambda i: (i, 0))
    second = pl.BlockSpec((rows, width), lambda i: (i + steps, 0))
    half = jax.ShapeDtypeStruct((total // 2, width), left.dtype)
    return pl.pallas_call(
        halves_kernel,
        out_shape=(half, half),
        grid=(steps,),
        in_specs=[first, second],
        out_specs=(first, first),
        compiler_params=pltpu.CompilerParams(vmem_limit_bytes=8 * 2**20),
        cost_estimate=pl.CostEstimate(
            flops=10**6, bytes_accessed=2 * left.size * 2, transcendentals=0
        ),
        name="halves",
    )(left, right)


def combine_kernel(returned_ref, target_ref, share_ref, after_ref, out_ref):
    rows = after_ref.shape[0]
    total = after_ref[...].astype(jnp.float32)
    slot = lax.broadcasted_iota(jnp.int32, (rows, returned_ref.shape[0]), 1)
    mix = 0.0
    for k in range(TOP_K):
        chosen = (slot == target_ref[:, k : k + 1]).astype(jnp.bfloat16)
        picked = jnp.dot(chosen, returned_ref[...], preferred_element_type=jnp.float32)
        mix = mix + share_ref[:, k : k + 1] * picked
    out = (total + mix).astype(jnp.bfloat16)
    for t in range(out_ref.shape[0]):
        out_ref[t] = out


def combine(returned, target, share, after, copies):
    return pl.pallas_call(
        combine_kernel,
        out_shape=jax.ShapeDtypeStruct((copies, *after.shape), jnp.bfloat16),
        in_specs=[VECTORS] * 4,
        out_specs=VECTORS,
        compiler_params=pltpu.CompilerParams(vmem_limit_bytes=16 * 2**20),
        cost_estimate=pl.CostEstimate(
            flops=4 * returned.size * after.shape[0], bytes_accessed=10**6, transcendentals=0
        ),
        name="combine",
    )(returned, target, share, after)


def assemble_kernel(columns_ref, out_ref, semaphores):
    copies = []
    for t in range(columns_ref.shape[0]):
        target = out_ref.at[:, t * LANES : (t + 1) * LANES]
        copies.append(pltpu.make_async_copy(columns_ref.at[t], target, semaphores.at[t]))
    for copy in copies:
        copy.start()
    for copy in copies:
        copy.wait()


def assemble(columns):
    count, total, lanes = columns.shape
    return pl.pallas_call(
        assemble_kernel,
        out_shape=jax.ShapeDtypeStruct((total, count * lanes), columns.dtype),
        in_specs=[VECTORS],
        out_specs=ANYWHERE,
        scratch_shapes=[pltpu.SemaphoreType.DMA((count,))],
        compiler_params=pltpu.CompilerParams(vmem_limit_bytes=4 * 2**20),
        name="assemble",
    )(columns)


def layer(
    residual_in,
    mix_gain,
    pool_weight,
    pool_scale,
    ffn_gain,
    route_ids,
    route_weights,
    gate_weight,
    up_weight,
    down_weight,
):
    tp_count = lax.axis_size(TP)
    sp_count = lax.axis_size(SP)
    tp_index = lax.axis_index(TP)
    sp_index = lax.axis_index(SP)
    tok_count, width = residual_in.shape
    col_count = pool_weight.shape[1]
    slots = tok_count // ROWS * CAP
    group_index = tp_index * col_count * GROUPS // width

    own = jnp.concatenate([gate_weight[0].T, up_weight[0].T, down_weight[0]], axis=0)
    left = from_quad(own, 1)
    right = from_quad(own, -1)
    rim = from_behind(residual_in[tok_count - SPAN :], SP, 1)

    index = jnp.stack([group_index, tp_index, sp_index]).astype(jnp.int32)
    outgoing, after, target = mixer(
        index, route_ids.T, residual_in, rim, mix_gain, pool_weight, pool_scale, sp_count
    )
    outgoing = outgoing.reshape(sp_count, slots, col_count)
    arrived = lax.all_to_all(outgoing, SP, 0, 0, tiled=True)
    upper, lower = halves(left, right)
    upper = from_quad(upper, 1)
    lower = from_quad(lower, -1)
    arrived = arrived.reshape(sp_count * slots, col_count)

    side = lax.axis_size("x")
    core = lax.axis_index("c").astype(jnp.int32).reshape(1)
    quarter = arrived.reshape(1, side, -1, col_count)
    quarter = jnp.broadcast_to(quarter, (side, *quarter.shape[1:]))
    gathered = exchange(quarter.reshape(tp_count, -1, col_count))
    term = expert(gathered, core, ffn_gain, [own, left, right, upper, lower], side)
    summed = exchange(term).reshape(quarter.shape)
    expert_out = jnp.sum(summed.astype(jnp.float32), axis=0).astype(jnp.bfloat16)
    returned = lax.all_to_all(
        expert_out.reshape(sp_count, slots, col_count), SP, 0, 0, tiled=True
    ).reshape(sp_count * slots, col_count)
    copies = combine(returned, target.T, route_weights, after, tp_count)
    columns = lax.all_to_all(copies, TP, 0, 0, tiled=True)
    return assemble(columns)


def solution(mesh):
    torus = Mesh(mesh.devices.reshape(-1, 2, 4, mesh.shape["tp"] // 4), ALL)
    return jax.shard_map(
        layer,
        mesh=torus,
        in_specs=(
            P(SP, None),
            P(),
            P(None, TP),
            P(TP),
            P(),
            P(SP, None),
            P(SP, None),
            P(SP, None, TP),
            P(SP, None, TP),
            P(SP, TP, None),
        ),
        out_specs=P(SP, None),
        check_vma=False,
    )
```

```python
import functools
import math

import jax
import jax.numpy as jnp
import numpy as np
from jax import lax
from jax.experimental import pallas as pl
from jax.experimental.pallas import tpu as pltpu
from jax.sharding import Mesh
from jax.sharding import PartitionSpec as P

GROUPS = 4
SPAN = 16
TOP_K = 2
ROWS = 16
CAP = 2
SP = ("z", "c")
TP = ("y", "x")
ALL = ("z", "c", "y", "x")

EPS = 1e-06
LANES = 128


def from_behind(value, axis, steps):
    count = lax.axis_size(axis)
    first, last = (max(0, -steps), min(count, count - steps))
    return lax.ppermute(value, axis, [(source, source + steps) for source in range(first, last)])


def planes():
    sizes = [lax.axis_size(a) for a in ALL]
    index = np.arange(math.prod(sizes)).reshape(sizes)
    return [
        index[z, c] if c % 2 == 0 else index[z, c].T
        for z in range(sizes[0])
        for c in range(sizes[1])
    ]


def from_quad(value, steps):
    pairs = []
    for plane in planes():
        pairs += list(zip(plane.ravel().tolist(), np.roll(plane, -steps, axis=1).ravel().tolist()))
    return lax.ppermute(value, ALL, pairs)


def exchange(blocks):
    groups = [plane.ravel().tolist() for plane in planes()]
    return lax.all_to_all(blocks, ALL, 0, 0, tiled=True, axis_index_groups=groups)


def place(t, side, swapped):
    return jnp.where(swapped == 0, t, (t % side) * side + t // side)


def expert_kernel(side, core_ref, x_ref, gain_ref, *refs):
    pieces = (len(refs) - 3) // 3 * 2
    sources, out_ref, normed_ref = (refs[:pieces], refs[pieces], refs[pieces + 1])
    weights, semaphores = (refs[pieces + 2 : -1], refs[-1])
    copies = []
    for i, source in enumerate(sources):
        height = source.shape[0]
        target = weights[i // 2].at[i % 2 * height : (i % 2 + 1) * height]
        copies.append(pltpu.make_async_copy(source, target, semaphores.at[i]))
    for copy in copies:
        copy.start()
    count, rows, lanes = x_ref.shape
    squares = jnp.zeros((rows, lanes), jnp.float32)
    for t in range(count):
        values = x_ref[t].astype(jnp.float32)
        squares = squares + values * values
    inverse = lax.rsqrt(jnp.sum(squares, axis=1, keepdims=True) / (count * lanes) + EPS)
    for t in range(count):
        columns = slice(t * lanes, (t + 1) * lanes)
        values = x_ref[place(t, side, core_ref[0])].astype(jnp.float32)
        normed_ref[:, columns] = (values * inverse * gain_ref[:, columns]).astype(jnp.bfloat16)
    units = weights[0].shape[0] // 3
    contract = (((1,), (1,)), ((), ()))
    normed = normed_ref[...]
    hidden, downs = ([], [])
    for i, ref in enumerate(weights):
        copies[2 * i].wait()
        copies[2 * i + 1].wait()
        gate_rows, up_rows = (ref[:units], ref[units : 2 * units])
        downs.append(ref.at[2 * units :])
        gate = lax.dot_general(normed, gate_rows, contract, preferred_element_type=jnp.float32)
        up = lax.dot_general(normed, up_rows, contract, preferred_element_type=jnp.float32)
        hidden.append((gate * (1.0 / (1.0 + jnp.exp(-gate))) * up).astype(jnp.bfloat16))
    for t in range(0, count, 2):
        total = 0.0
        for part, down in zip(hidden, downs):
            total = total + jnp.dot(
                part,
                down[:, t * lanes : (t + 2) * lanes],
                preferred_element_type=jnp.float32,
            )
        total = total.astype(jnp.bfloat16)
        out_ref[place(t, side, core_ref[0])] = total[:, :lanes]
        out_ref[place(t + 1, side, core_ref[0])] = total[:, lanes:]


SCALARS = pl.BlockSpec(memory_space=pltpu.SMEM)
VECTORS = pl.BlockSpec(memory_space=pltpu.VMEM)
ANYWHERE = pl.BlockSpec(memory_space=pl.ANY)


def expert(blocks, core, gain, weights, side):
    count, rows, lanes = blocks.shape
    width = count * lanes
    slices = len(weights) // 2
    height = 2 * weights[0].shape[0]
    units = height // 3
    return pl.pallas_call(
        functools.partial(expert_kernel, side),
        out_shape=jax.ShapeDtypeStruct(blocks.shape, jnp.bfloat16),
        in_specs=[SCALARS, VECTORS, VECTORS] + [ANYWHERE] * len(weights),
        out_specs=VECTORS,
        scratch_shapes=[pltpu.VMEM((rows, width), jnp.bfloat16)]
        + [pltpu.VMEM((height, width), jnp.bfloat16)] * slices
        + [pltpu.SemaphoreType.DMA((len(weights),))],
        compiler_params=pltpu.CompilerParams(vmem_limit_bytes=32 * 2**20),
        cost_estimate=pl.CostEstimate(
            flops=6 * rows * units * width * side,
            bytes_accessed=6 * units * width * side,
            transcendentals=rows * units * side,
        ),
        name="expert",
    )(core, blocks, gain[None], *weights)


def inverse_rms(ref):
    rows, width = ref.shape
    squares = jnp.zeros((rows, LANES), jnp.float32)
    for first in range(0, width, LANES):
        values = ref[:, first : first + LANES].astype(jnp.float32)
        squares = squares + values * values
    return lax.rsqrt(jnp.sum(squares, axis=1, keepdims=True) / width + EPS)


def mixer_kernel(
    experts,
    index_ref,
    ids_ref,
    x_ref,
    rim_ref,
    gain_ref,
    weight_ref,
    scale_ref,
    outgoing_ref,
    after_ref,
    target_ref,
):
    group, tp_index, sp_index = (index_ref[0], index_ref[1], index_ref[2])
    rows = x_ref.shape[0]
    span = rim_ref.shape[0]
    group_width, col_count = weight_ref.shape
    columns = pl.ds(pl.multiple_of(group * group_width, group_width), group_width)
    gain = gain_ref[:, columns]

    def normed(ref):
        return (ref[:, columns].astype(jnp.float32) * inverse_rms(ref) * gain).astype(jnp.bfloat16)

    window = jnp.left_shift(2, group)
    here = normed(x_ref)
    row = lax.broadcasted_iota(jnp.int32, (rows, rows), 0)
    col = lax.broadcasted_iota(jnp.int32, (rows, rows), 1)
    band = ((col <= row) & (row - col < window)).astype(jnp.bfloat16)
    sums = jnp.dot(band, here, preferred_element_type=jnp.float32)
    behind = lax.broadcasted_iota(jnp.int32, (rows, span), 0) + span
    behind = behind - lax.broadcasted_iota(jnp.int32, (rows, span), 1)
    sums = sums + jnp.dot(
        (behind < window).astype(jnp.bfloat16), normed(rim_ref), preferred_element_type=jnp.float32
    )
    position = sp_index * rows + lax.broadcasted_iota(jnp.int32, (rows, 1), 0)
    divisor = jnp.minimum(position + 1, window).astype(jnp.float32)
    pooled = (sums / divisor - here.astype(jnp.float32)).astype(jnp.bfloat16)
    mixed = jnp.dot(pooled, weight_ref[...], preferred_element_type=jnp.float32) * scale_ref[...]
    own = pl.ds(pl.multiple_of(tp_index * col_count, col_count), col_count)
    stream = x_ref[:, own].astype(jnp.float32)
    after = (stream + mixed.astype(jnp.bfloat16).astype(jnp.float32)).astype(jnp.bfloat16)
    after_ref[...] = after

    ids = ids_ref[...]
    expert_index = lax.broadcasted_iota(jnp.int32, (experts, rows), 0)
    named = [(ids[k : k + 1] == expert_index).astype(jnp.float32) for k in range(TOP_K)]
    earlier = ((row // ROWS == col // ROWS) & (row < col)).astype(jnp.bfloat16)
    before = jnp.dot(
        sum(named).astype(jnp.bfloat16), earlier, preferred_element_type=jnp.float32
    )
    slots = rows // ROWS * CAP
    block = lax.broadcasted_iota(jnp.int32, (1, rows), 1) // ROWS * CAP
    targets = []
    for k in range(TOP_K):
        slot = jnp.sum(before * named[k], axis=0, keepdims=True).astype(jnp.int32)
        targets.append(ids[k : k + 1] * slots + block + slot)
        target_ref[k : k + 1] = targets[k]
    for first in range(0, experts * slots, rows):
        place_here = row + first
        chosen = (place_here == targets[0]) | (place_here == targets[1])
        outgoing_ref[first : first + rows] = jnp.dot(
            chosen.astype(jnp.bfloat16), after, preferred_element_type=jnp.float32
        ).astype(jnp.bfloat16)


def mixer(index, ids, x, rim, gain, weight, scale, experts):
    rows = x.shape[0]
    col_count = weight.shape[1]
    slots = rows // ROWS * CAP
    return pl.pallas_call(
        functools.partial(mixer_kernel, experts),
        out_shape=(
            jax.ShapeDtypeStruct((experts * slots, col_count), jnp.bfloat16),
            jax.ShapeDtypeStruct((rows, col_count), jnp.bfloat16),
            jax.ShapeDtypeStruct((TOP_K, rows), jnp.int32),
        ),
        in_specs=[SCALARS] + [VECTORS] * 6,
        out_specs=(VECTORS,) * 3,
        compiler_params=pltpu.CompilerParams(vmem_limit_bytes=16 * 2**20),
        cost_estimate=pl.CostEstimate(
            flops=10**9, bytes_accessed=4 * x.size, transcendentals=rows
        ),
        name="mixer",
    )(index, ids, x, rim, gain[None], weight, scale[None])


def combine_kernel(returned_ref, target_ref, share_ref, after_ref, out_ref):
    rows = after_ref.shape[0]
    total = after_ref[...].astype(jnp.float32)
    slot = lax.broadcasted_iota(jnp.int32, (rows, returned_ref.shape[0]), 1)
    mix = 0.0
    for k in range(TOP_K):
        chosen = (slot == target_ref[:, k : k + 1]).astype(jnp.bfloat16)
        picked = jnp.dot(chosen, returned_ref[...], preferred_element_type=jnp.float32)
        mix = mix + share_ref[:, k : k + 1] * picked
    out = (total + mix).astype(jnp.bfloat16)
    for t in range(out_ref.shape[0]):
        out_ref[t] = out


def combine(returned, target, share, after, copies):
    return pl.pallas_call(
        combine_kernel,
        out_shape=jax.ShapeDtypeStruct((copies, *after.shape), jnp.bfloat16),
        in_specs=[VECTORS] * 4,
        out_specs=VECTORS,
        compiler_params=pltpu.CompilerParams(vmem_limit_bytes=16 * 2**20),
        cost_estimate=pl.CostEstimate(
            flops=4 * returned.size * after.shape[0], bytes_accessed=10**6, transcendentals=0
        ),
        name="combine",
    )(returned, target, share, after)


def assemble_kernel(columns_ref, out_ref, semaphores):
    copies = []
    for t in range(columns_ref.shape[0]):
        target = out_ref.at[:, t * LANES : (t + 1) * LANES]
        copies.append(pltpu.make_async_copy(columns_ref.at[t], target, semaphores.at[t]))
    for copy in copies:
        copy.start()
    for copy in copies:
        copy.wait()


def assemble(columns):
    count, total, lanes = columns.shape
    return pl.pallas_call(
        assemble_kernel,
        out_shape=jax.ShapeDtypeStruct((total, count * lanes), columns.dtype),
        in_specs=[VECTORS],
        out_specs=ANYWHERE,
        scratch_shapes=[pltpu.SemaphoreType.DMA((count,))],
        compiler_params=pltpu.CompilerParams(vmem_limit_bytes=4 * 2**20),
        name="assemble",
    )(columns)


def layer(
    residual_in,
    mix_gain,
    pool_weight,
    pool_scale,
    ffn_gain,
    route_ids,
    route_weights,
    gate_weight,
    up_weight,
    down_weight,
):
    tp_count = lax.axis_size(TP)
    sp_count = lax.axis_size(SP)
    tp_index = lax.axis_index(TP)
    sp_index = lax.axis_index(SP)
    tok_count, width = residual_in.shape
    col_count = pool_weight.shape[1]
    slots = tok_count // ROWS * CAP
    group_index = tp_index * col_count * GROUPS // width

    middle = up_weight.shape[2] // 2
    up_t = up_weight[0].T
    top = jnp.concatenate([gate_weight[0].T, up_t[:middle]], axis=0)
    bottom = jnp.concatenate([up_t[middle:], down_weight[0]], axis=0)
    left_top, right_bottom = (from_quad(top, 1), from_quad(bottom, -1))
    left_bottom, right_top = (from_quad(bottom, 1), from_quad(top, -1))
    rim = from_behind(residual_in[tok_count - SPAN :], SP, 1)

    index = jnp.stack([group_index, tp_index, sp_index]).astype(jnp.int32)
    outgoing, after, target = mixer(
        index, route_ids.T, residual_in, rim, mix_gain, pool_weight, pool_scale, sp_count
    )
    outgoing = outgoing.reshape(sp_count, slots, col_count)
    arrived = lax.all_to_all(outgoing, SP, 0, 0, tiled=True)
    far_top, far_bottom = (from_quad(left_top, 1), from_quad(right_bottom, -1))

    side = lax.axis_size("x")
    core = lax.axis_index("c").astype(jnp.int32).reshape(1)
    quarter = arrived.reshape(1, side, -1, col_count)
    quarter = jnp.broadcast_to(quarter, (side, *quarter.shape[1:]))
    gathered = exchange(quarter.reshape(tp_count, -1, col_count))
    term = expert(gathered, core, ffn_gain, [top, bottom, left_top, left_bottom, right_top, right_bottom, far_top, far_bottom], side)
    summed = exchange(term).reshape(quarter.shape)
    expert_out = jnp.sum(summed.astype(jnp.float32), axis=0).astype(jnp.bfloat16)
    returned = lax.all_to_all(
        expert_out.reshape(sp_count, slots, col_count), SP, 0, 0, tiled=True
    ).reshape(sp_count * slots, col_count)
    copies = combine(returned, target.T, route_weights, after, tp_count)
    columns = lax.all_to_all(copies, TP, 0, 0, tiled=True)
    return assemble(columns)


def solution(mesh):
    torus = Mesh(mesh.devices.reshape(-1, 2, 4, mesh.shape["tp"] // 4), ALL)
    return jax.shard_map(
        layer,
        mesh=torus,
        in_specs=(
            P(SP, None),
            P(),
            P(None, TP),
            P(TP),
            P(),
            P(SP, None),
            P(SP, None),
            P(SP, None, TP),
            P(SP, None, TP),
            P(SP, TP, None),
        ),
        out_specs=P(SP, None),
        check_vma=False,
    )
```

```python
import functools
import math

import jax
import jax.numpy as jnp
import numpy as np
from jax import lax
from jax.experimental import pallas as pl
from jax.experimental.pallas import tpu as pltpu
from jax.sharding import Mesh
from jax.sharding import PartitionSpec as P

GROUPS = 4
SPAN = 16
TOP_K = 2
ROWS = 16
CAP = 2
SP = ("z", "c")
TP = ("y", "x")
ALL = ("z", "c", "y", "x")

EPS = 1e-06
LANES = 128


def from_behind(value, axis, steps):
    count = lax.axis_size(axis)
    first, last = (max(0, -steps), min(count, count - steps))
    return lax.ppermute(value, axis, [(source, source + steps) for source in range(first, last)])


def planes():
    sizes = [lax.axis_size(a) for a in ALL]
    index = np.arange(math.prod(sizes)).reshape(sizes)
    return [
        index[z, c] if c % 2 == 0 else index[z, c].T
        for z in range(sizes[0])
        for c in range(sizes[1])
    ]


def from_quad(value, steps):
    pairs = []
    for plane in planes():
        pairs += list(zip(plane.ravel().tolist(), np.roll(plane, -steps, axis=1).ravel().tolist()))
    return lax.ppermute(value, ALL, pairs)


def exchange(blocks):
    groups = [plane.ravel().tolist() for plane in planes()]
    return lax.all_to_all(blocks, ALL, 0, 0, tiled=True, axis_index_groups=groups)


def place(t, side, swapped):
    return jnp.where(swapped == 0, t, (t % side) * side + t // side)


def expert_kernel(side, core_ref, x_ref, gain_ref, *refs):
    pieces = (len(refs) - 3) // 3 * 2
    sources, out_ref, normed_ref = (refs[:pieces], refs[pieces], refs[pieces + 1])
    weights, semaphores = (refs[pieces + 2 : -1], refs[-1])
    copies = []
    for i, source in enumerate(sources):
        height = source.shape[0]
        target = weights[i // 2].at[i % 2 * height : (i % 2 + 1) * height]
        copies.append(pltpu.make_async_copy(source, target, semaphores.at[i]))
    for copy in copies:
        copy.start()
    count, rows, lanes = x_ref.shape
    squares = jnp.zeros((rows, lanes), jnp.float32)
    for t in range(count):
        values = x_ref[t].astype(jnp.float32)
        squares = squares + values * values
    inverse = lax.rsqrt(jnp.sum(squares, axis=1, keepdims=True) / (count * lanes) + EPS)
    for t in range(count):
        columns = slice(t * lanes, (t + 1) * lanes)
        values = x_ref[place(t, side, core_ref[0])].astype(jnp.float32)
        normed_ref[:, columns] = (values * inverse * gain_ref[:, columns]).astype(jnp.bfloat16)
    units = weights[0].shape[0] // 3
    contract = (((1,), (1,)), ((), ()))
    normed = normed_ref[...]
    hidden, downs = ([], [])
    for i, ref in enumerate(weights):
        copies[2 * i].wait()
        copies[2 * i + 1].wait()
        gate_rows, up_rows = (ref[:units], ref[units : 2 * units])
        downs.append(ref.at[2 * units :])
        gate = lax.dot_general(normed, gate_rows, contract, preferred_element_type=jnp.float32)
        up = lax.dot_general(normed, up_rows, contract, preferred_element_type=jnp.float32)
        hidden.append((gate * (1.0 / (1.0 + jnp.exp(-gate))) * up).astype(jnp.bfloat16))
    for t in range(0, count, 2):
        total = 0.0
        for part, down in zip(hidden, downs):
            total = total + jnp.dot(
                part,
                down[:, t * lanes : (t + 2) * lanes],
                preferred_element_type=jnp.float32,
            )
        total = total.astype(jnp.bfloat16)
        out_ref[place(t, side, core_ref[0])] = total[:, :lanes]
        out_ref[place(t + 1, side, core_ref[0])] = total[:, lanes:]


SCALARS = pl.BlockSpec(memory_space=pltpu.SMEM)
VECTORS = pl.BlockSpec(memory_space=pltpu.VMEM)
ANYWHERE = pl.BlockSpec(memory_space=pl.ANY)
FAR = pl.BlockSpec(memory_space=pltpu.HBM)


def expert(blocks, core, gain, weights, side):
    count, rows, lanes = blocks.shape
    width = count * lanes
    slices = len(weights) // 2
    height = 2 * weights[0].shape[0]
    units = height // 3
    return pl.pallas_call(
        functools.partial(expert_kernel, side),
        out_shape=jax.ShapeDtypeStruct(blocks.shape, jnp.bfloat16),
        in_specs=[SCALARS, VECTORS, VECTORS] + [ANYWHERE] * len(weights),
        out_specs=VECTORS,
        scratch_shapes=[pltpu.VMEM((rows, width), jnp.bfloat16)]
        + [pltpu.VMEM((height, width), jnp.bfloat16)] * slices
        + [pltpu.SemaphoreType.DMA((len(weights),))],
        compiler_params=pltpu.CompilerParams(vmem_limit_bytes=32 * 2**20),
        cost_estimate=pl.CostEstimate(
            flops=6 * rows * units * width * side,
            bytes_accessed=6 * units * width * side,
            transcendentals=rows * units * side,
        ),
        name="expert",
    )(core, blocks, gain[None], *weights)


def inverse_rms(ref, copies=()):
    rows, width = ref.shape
    squares = jnp.zeros((rows, LANES), jnp.float32)
    for first in range(0, width, LANES):
        if copies and first % (width // len(copies)) == 0:
            copies[first * len(copies) // width].wait()
        values = ref[:, first : first + LANES].astype(jnp.float32)
        squares = squares + values * values
    return lax.rsqrt(jnp.sum(squares, axis=1, keepdims=True) / width + EPS)


def mixer_kernel(
    experts,
    index_ref,
    ids_ref,
    share_ref,
    source_ref,
    rim_ref,
    gain_ref,
    weight_ref,
    scale_ref,
    outgoing_ref,
    after_ref,
    plan_ref,
    x_ref,
    semaphores,
):
    copies = []
    part = source_ref.shape[1] // semaphores.shape[0]
    for i in range(semaphores.shape[0]):
        columns = slice(i * part, (i + 1) * part)
        copies.append(
            pltpu.make_async_copy(source_ref.at[:, columns], x_ref.at[:, columns], semaphores.at[i])
        )
    for copy in copies:
        copy.start()
    group, tp_index, sp_index = (index_ref[0], index_ref[1], index_ref[2])
    rows = x_ref.shape[0]
    span = rim_ref.shape[0]
    group_width, col_count = weight_ref.shape
    columns = pl.ds(pl.multiple_of(group * group_width, group_width), group_width)
    gain = gain_ref[:, columns]

    def normed(ref, inverse):
        return (ref[:, columns].astype(jnp.float32) * inverse * gain).astype(jnp.bfloat16)

    window = jnp.left_shift(2, group)
    here = normed(x_ref, inverse_rms(x_ref, copies))
    row = lax.broadcasted_iota(jnp.int32, (rows, rows), 0)
    col = lax.broadcasted_iota(jnp.int32, (rows, rows), 1)
    band = ((col <= row) & (row - col < window)).astype(jnp.bfloat16)
    sums = jnp.dot(band, here, preferred_element_type=jnp.float32)
    behind = lax.broadcasted_iota(jnp.int32, (rows, span), 0) + span
    behind = behind - lax.broadcasted_iota(jnp.int32, (rows, span), 1)
    sums = sums + jnp.dot(
        (behind < window).astype(jnp.bfloat16), normed(rim_ref, inverse_rms(rim_ref)), preferred_element_type=jnp.float32
    )
    position = sp_index * rows + lax.broadcasted_iota(jnp.int32, (rows, 1), 0)
    divisor = jnp.minimum(position + 1, window).astype(jnp.float32)
    pooled = (sums / divisor - here.astype(jnp.float32)).astype(jnp.bfloat16)
    mixed = jnp.dot(pooled, weight_ref[...], preferred_element_type=jnp.float32) * scale_ref[...]
    own = pl.ds(pl.multiple_of(tp_index * col_count, col_count), col_count)
    stream = x_ref[:, own].astype(jnp.float32)
    after = (stream + mixed.astype(jnp.bfloat16).astype(jnp.float32)).astype(jnp.bfloat16)
    after_ref[...] = after

    ids = ids_ref[...]
    expert_index = lax.broadcasted_iota(jnp.int32, (experts, rows), 0)
    named = [(ids[k : k + 1] == expert_index).astype(jnp.float32) for k in range(TOP_K)]
    earlier = ((row // ROWS == col // ROWS) & (row < col)).astype(jnp.bfloat16)
    before = jnp.dot(
        sum(named).astype(jnp.bfloat16), earlier, preferred_element_type=jnp.float32
    )
    slots = rows // ROWS * CAP
    block = lax.broadcasted_iota(jnp.int32, (1, rows), 1) // ROWS * CAP
    targets = []
    for k in range(TOP_K):
        slot = jnp.sum(before * named[k], axis=0, keepdims=True).astype(jnp.int32)
        targets.append(ids[k : k + 1] * slots + block + slot)
    spare = jnp.zeros((8 - 2 * TOP_K, rows), jnp.float32)
    plan = [target.astype(jnp.float32) for target in targets] + [share_ref[...], spare]
    plan_ref[...] = jnp.concatenate(plan, axis=0).T
    for first in range(0, experts * slots, rows):
        place_here = row + first
        chosen = (place_here == targets[0]) | (place_here == targets[1])
        outgoing_ref[first : first + rows] = jnp.dot(
            chosen.astype(jnp.bfloat16), after, preferred_element_type=jnp.float32
        ).astype(jnp.bfloat16)


def mixer(index, ids, share, x, rim, gain, weight, scale, experts):
    rows = x.shape[0]
    col_count = weight.shape[1]
    slots = rows // ROWS * CAP
    return pl.pallas_call(
        functools.partial(mixer_kernel, experts),
        out_shape=(
            jax.ShapeDtypeStruct((experts * slots, col_count), jnp.bfloat16),
            jax.ShapeDtypeStruct((rows, col_count), jnp.bfloat16),
            jax.ShapeDtypeStruct((rows, 8), jnp.float32),
        ),
        in_specs=[SCALARS, VECTORS, VECTORS, FAR] + [VECTORS] * 4,
        out_specs=(VECTORS,) * 3,
        scratch_shapes=[pltpu.VMEM(x.shape, x.dtype), pltpu.SemaphoreType.DMA((GROUPS,))],
        compiler_params=pltpu.CompilerParams(vmem_limit_bytes=16 * 2**20),
        cost_estimate=pl.CostEstimate(
            flops=10**9, bytes_accessed=4 * x.size, transcendentals=rows
        ),
        name="mixer",
    )(index, ids, share, x, rim, gain[None], weight, scale[None])


def combine_kernel(returned_ref, plan_ref, after_ref, out_ref):
    rows = after_ref.shape[0]
    total = after_ref[...].astype(jnp.float32)
    slot = lax.broadcasted_iota(jnp.int32, (rows, returned_ref.shape[0]), 1)
    mix = 0.0
    for k in range(TOP_K):
        chosen = (slot == plan_ref[:, k : k + 1].astype(jnp.int32)).astype(jnp.bfloat16)
        picked = jnp.dot(chosen, returned_ref[...], preferred_element_type=jnp.float32)
        mix = mix + plan_ref[:, TOP_K + k : TOP_K + k + 1] * picked
    out = (total + mix).astype(jnp.bfloat16)
    for t in range(out_ref.shape[0]):
        out_ref[t] = out


def combine(returned, plan, after, copies):
    return pl.pallas_call(
        combine_kernel,
        out_shape=jax.ShapeDtypeStruct((copies, *after.shape), jnp.bfloat16),
        in_specs=[VECTORS] * 3,
        out_specs=VECTORS,
        compiler_params=pltpu.CompilerParams(vmem_limit_bytes=16 * 2**20),
        cost_estimate=pl.CostEstimate(
            flops=4 * returned.size * after.shape[0], bytes_accessed=10**6, transcendentals=0
        ),
        name="combine",
    )(returned, plan, after)


def assemble_kernel(columns_ref, out_ref, semaphores):
    copies = []
    for t in range(columns_ref.shape[0]):
        target = out_ref.at[:, t * LANES : (t + 1) * LANES]
        copies.append(pltpu.make_async_copy(columns_ref.at[t], target, semaphores.at[t]))
    for copy in copies:
        copy.start()
    for copy in copies:
        copy.wait()


def assemble(columns):
    count, total, lanes = columns.shape
    return pl.pallas_call(
        assemble_kernel,
        out_shape=jax.ShapeDtypeStruct((total, count * lanes), columns.dtype),
        in_specs=[VECTORS],
        out_specs=ANYWHERE,
        scratch_shapes=[pltpu.SemaphoreType.DMA((count,))],
        compiler_params=pltpu.CompilerParams(vmem_limit_bytes=4 * 2**20),
        name="assemble",
    )(columns)


def layer(
    residual_in,
    mix_gain,
    pool_weight,
    pool_scale,
    ffn_gain,
    route_ids,
    route_weights,
    gate_weight,
    up_weight,
    down_weight,
):
    tp_count = lax.axis_size(TP)
    sp_count = lax.axis_size(SP)
    tp_index = lax.axis_index(TP)
    sp_index = lax.axis_index(SP)
    tok_count, width = residual_in.shape
    col_count = pool_weight.shape[1]
    slots = tok_count // ROWS * CAP
    group_index = tp_index * col_count * GROUPS // width

    middle = up_weight.shape[2] // 2
    up_t = up_weight[0].T
    top = jnp.concatenate([gate_weight[0].T, up_t[:middle]], axis=0)
    bottom = jnp.concatenate([up_t[middle:], down_weight[0]], axis=0)
    left_top, right_bottom = (from_quad(top, 1), from_quad(bottom, -1))
    left_bottom, right_top = (from_quad(bottom, 1), from_quad(top, -1))
    rim = from_behind(residual_in[tok_count - SPAN :], SP, 1)

    index = jnp.stack([group_index, tp_index, sp_index]).astype(jnp.int32)
    outgoing, after, plan = mixer(
        index,
        route_ids.T,
        route_weights.T,
        residual_in,
        rim,
        mix_gain,
        pool_weight,
        pool_scale,
        sp_count,
    )
    outgoing = outgoing.reshape(sp_count, slots, col_count)
    arrived = lax.all_to_all(outgoing, SP, 0, 0, tiled=True)
    far_top, far_bottom = (from_quad(left_top, 1), from_quad(right_bottom, -1))

    side = lax.axis_size("x")
    core = lax.axis_index("c").astype(jnp.int32).reshape(1)
    quarter = arrived.reshape(1, side, -1, col_count)
    quarter = jnp.broadcast_to(quarter, (side, *quarter.shape[1:]))
    gathered = exchange(quarter.reshape(tp_count, -1, col_count))
    term = expert(gathered, core, ffn_gain, [top, bottom, left_top, left_bottom, right_top, right_bottom, far_top, far_bottom], side)
    summed = exchange(term).reshape(quarter.shape)
    expert_out = jnp.sum(summed.astype(jnp.float32), axis=0).astype(jnp.bfloat16)
    returned = lax.all_to_all(
        expert_out.reshape(sp_count, slots, col_count), SP, 0, 0, tiled=True
    ).reshape(sp_count * slots, col_count)
    copies = combine(returned, plan, after, tp_count)
    columns = lax.all_to_all(copies, TP, 0, 0, tiled=True)
    return assemble(columns)


def solution(mesh):
    torus = Mesh(mesh.devices.reshape(-1, 2, 4, mesh.shape["tp"] // 4), ALL)
    return jax.shard_map(
        layer,
        mesh=torus,
        in_specs=(
            P(SP, None),
            P(),
            P(None, TP),
            P(TP),
            P(),
            P(SP, None),
            P(SP, None),
            P(SP, None, TP),
            P(SP, None, TP),
            P(SP, TP, None),
        ),
        out_specs=P(SP, None),
        check_vma=False,
    )
```

```python
import functools
import math

import jax
import jax.numpy as jnp
import numpy as np
from jax import lax
from jax.experimental import pallas as pl
from jax.experimental.pallas import tpu as pltpu
from jax.sharding import Mesh
from jax.sharding import PartitionSpec as P

GROUPS = 4
SPAN = 16
TOP_K = 2
ROWS = 16
CAP = 2
SP = ("z", "c")
TP = ("y", "x")
ALL = ("z", "c", "y", "x")


EPS = 1e-06
LANES = 128


def from_behind(value, axis, steps):
    count = lax.axis_size(axis)
    first, last = (max(0, -steps), min(count, count - steps))
    return lax.ppermute(value, axis, [(source, source + steps) for source in range(first, last)])


def planes():
    sizes = [lax.axis_size(a) for a in ALL]
    index = np.arange(math.prod(sizes)).reshape(sizes)
    return [
        index[z, c] if c % 2 == 0 else index[z, c].T
        for z in range(sizes[0])
        for c in range(sizes[1])
    ]


def from_quad(value, steps):
    pairs = []
    for plane in planes():
        pairs += list(zip(plane.ravel().tolist(), np.roll(plane, -steps, axis=1).ravel().tolist()))
    return lax.ppermute(value, ALL, pairs)


def from_mate(value, steps):
    sizes = [lax.axis_size(a) for a in ALL]
    index = np.arange(math.prod(sizes)).reshape(sizes)
    pairs = []
    for number, plane in enumerate(planes()):
        owners = index[number // sizes[1], number % sizes[1]]
        pairs += list(zip(np.roll(owners, steps, axis=1).ravel().tolist(), plane.ravel().tolist()))
    return lax.ppermute(value, ALL, pairs)


def exchange(blocks, across=False):
    if across:
        groups = [column for plane in planes() for column in plane.T.tolist()]
    else:
        groups = [plane.ravel().tolist() for plane in planes()]
    return lax.all_to_all(blocks, ALL, 0, 0, tiled=True, axis_index_groups=groups)


def come_back(blocks):
    groups = np.stack([plane.ravel() for plane in planes()], axis=1).tolist()
    return lax.all_to_all(blocks, ALL, 0, 0, tiled=True, axis_index_groups=groups)


def place(t, side, swapped):
    return jnp.where(swapped == 0, t, (t % side) * side + t // side)


def expert_kernel(side, core_ref, x_ref, gain_ref, *refs):
    pieces = (len(refs) - 3) // 3 * 2
    sources, out_ref, normed_ref = (refs[:pieces], refs[pieces], refs[pieces + 1])
    weights, semaphores = (refs[pieces + 2 : -1], refs[-1])
    copies = []
    for i, source in enumerate(sources):
        height = source.shape[0]
        target = weights[i // 2].at[i % 2 * height : (i % 2 + 1) * height]
        copies.append(pltpu.make_async_copy(source, target, semaphores.at[i]))
    for copy in copies:
        copy.start()
    count, rows, lanes = x_ref.shape
    squares = jnp.zeros((rows, lanes), jnp.float32)
    for t in range(count):
        values = x_ref[t].astype(jnp.float32)
        squares = squares + values * values
    inverse = lax.rsqrt(jnp.sum(squares, axis=1, keepdims=True) / (count * lanes) + EPS)
    for t in range(count):
        columns = slice(t * lanes, (t + 1) * lanes)
        values = x_ref[place(t, side, core_ref[0])].astype(jnp.float32)
        normed_ref[:, columns] = (values * inverse * gain_ref[:, columns]).astype(jnp.bfloat16)
    units = weights[0].shape[0] // 3
    contract = (((1,), (1,)), ((), ()))
    normed = normed_ref[...]
    hidden, downs = ([], [])
    for i, ref in enumerate(weights):
        copies[2 * i].wait()
        copies[2 * i + 1].wait()
        gate_rows, up_rows = (ref[:units], ref[units : 2 * units])
        downs.append(ref.at[2 * units :])
        gate = lax.dot_general(normed, gate_rows, contract, preferred_element_type=jnp.float32)
        up = lax.dot_general(normed, up_rows, contract, preferred_element_type=jnp.float32)
        hidden.append((gate * (1.0 / (1.0 + jnp.exp(-gate))) * up).astype(jnp.bfloat16))
    for t in range(0, count, 2):
        total = 0.0
        for part, down in zip(hidden, downs):
            total = total + jnp.dot(
                part,
                down[:, t * lanes : (t + 2) * lanes],
                preferred_element_type=jnp.float32,
            )
        total = total.astype(jnp.bfloat16)
        out_ref[t] = total[:, :lanes]
        out_ref[t + 1] = total[:, lanes:]


SCALARS = pl.BlockSpec(memory_space=pltpu.SMEM)
VECTORS = pl.BlockSpec(memory_space=pltpu.VMEM)
ANYWHERE = pl.BlockSpec(memory_space=pl.ANY)
FAR = pl.BlockSpec(memory_space=pltpu.HBM)


def expert(blocks, core, gain, weights, side):
    count, rows, lanes = blocks.shape
    width = count * lanes
    slices = len(weights) // 2
    height = 2 * weights[0].shape[0]
    units = height // 3
    return pl.pallas_call(
        functools.partial(expert_kernel, side),
        out_shape=jax.ShapeDtypeStruct(blocks.shape, jnp.bfloat16),
        in_specs=[SCALARS, VECTORS, VECTORS] + [ANYWHERE] * len(weights),
        out_specs=VECTORS,
        scratch_shapes=[pltpu.VMEM((rows, width), jnp.bfloat16)]
        + [pltpu.VMEM((height, width), jnp.bfloat16)] * slices
        + [pltpu.SemaphoreType.DMA((len(weights),))],
        compiler_params=pltpu.CompilerParams(vmem_limit_bytes=32 * 2**20),
        cost_estimate=pl.CostEstimate(
            flops=6 * rows * units * width * side,
            bytes_accessed=6 * units * width * side,
            transcendentals=rows * units * side,
        ),
        name="expert",
    )(core, blocks, gain[None], *weights)


def inverse_rms(ref, copies=()):
    rows, width = ref.shape
    squares = jnp.zeros((rows, LANES), jnp.float32)
    for first in range(0, width, LANES):
        if copies and first % (width // len(copies)) == 0:
            copies[first * len(copies) // width].wait()
        values = ref[:, first : first + LANES].astype(jnp.float32)
        squares = squares + values * values
    return lax.rsqrt(jnp.sum(squares, axis=1, keepdims=True) / width + EPS)


def mixer_kernel(
    experts,
    index_ref,
    ids_ref,
    share_ref,
    source_ref,
    rim_ref,
    gain_ref,
    weight_ref,
    scale_ref,
    outgoing_ref,
    plan_ref,
    *refs,
):
    part_refs, (x_ref, after_ref, semaphores) = (refs[:-3], refs[-3:])
    copies = []
    part = source_ref.shape[1] // semaphores.shape[0]
    for i in range(semaphores.shape[0]):
        columns = slice(i * part, (i + 1) * part)
        copies.append(
            pltpu.make_async_copy(source_ref.at[:, columns], x_ref.at[:, columns], semaphores.at[i])
        )
    for copy in copies:
        copy.start()
    group, tp_index, sp_index = (index_ref[0], index_ref[1], index_ref[2])
    rows = x_ref.shape[0]
    span = rim_ref.shape[0]
    group_width, col_count = weight_ref.shape
    columns = pl.ds(pl.multiple_of(group * group_width, group_width), group_width)
    gain = gain_ref[:, columns]

    def normed(ref, inverse):
        return (ref[:, columns].astype(jnp.float32) * inverse * gain).astype(jnp.bfloat16)

    window = jnp.left_shift(2, group)
    here = normed(x_ref, inverse_rms(x_ref, copies))
    row = lax.broadcasted_iota(jnp.int32, (rows, rows), 0)
    col = lax.broadcasted_iota(jnp.int32, (rows, rows), 1)
    band = ((col <= row) & (row - col < window)).astype(jnp.bfloat16)
    sums = jnp.dot(band, here, preferred_element_type=jnp.float32)
    behind = lax.broadcasted_iota(jnp.int32, (rows, span), 0) + span
    behind = behind - lax.broadcasted_iota(jnp.int32, (rows, span), 1)
    sums = sums + jnp.dot(
        (behind < window).astype(jnp.bfloat16), normed(rim_ref, inverse_rms(rim_ref)), preferred_element_type=jnp.float32
    )
    position = sp_index * rows + lax.broadcasted_iota(jnp.int32, (rows, 1), 0)
    divisor = jnp.minimum(position + 1, window).astype(jnp.float32)
    pooled = (sums / divisor - here.astype(jnp.float32)).astype(jnp.bfloat16)
    mixed = jnp.dot(pooled, weight_ref[...], preferred_element_type=jnp.float32) * scale_ref[...]
    own = pl.ds(pl.multiple_of(tp_index * col_count, col_count), col_count)
    stream = x_ref[:, own].astype(jnp.float32)
    after = (stream + mixed.astype(jnp.bfloat16).astype(jnp.float32)).astype(jnp.bfloat16)
    after_ref[...] = after
    height = rows // len(part_refs)
    for step, ref in enumerate(part_refs):
        quarter = (index_ref[3] + step) % len(part_refs)
        ref[...] = after_ref[pl.ds(pl.multiple_of(quarter * height, height), height)]

    ids = ids_ref[...]
    expert_index = lax.broadcasted_iota(jnp.int32, (experts, rows), 0)
    named = [(ids[k : k + 1] == expert_index).astype(jnp.float32) for k in range(TOP_K)]
    earlier = ((row // ROWS == col // ROWS) & (row < col)).astype(jnp.bfloat16)
    before = jnp.dot(
        sum(named).astype(jnp.bfloat16), earlier, preferred_element_type=jnp.float32
    )
    slots = rows // ROWS * CAP
    block = lax.broadcasted_iota(jnp.int32, (1, rows), 1) // ROWS * CAP
    targets = []
    for k in range(TOP_K):
        slot = jnp.sum(before * named[k], axis=0, keepdims=True).astype(jnp.int32)
        targets.append(ids[k : k + 1] * slots + block + slot)
    spare = jnp.zeros((8 - 2 * TOP_K, rows), jnp.float32)
    plan = [target.astype(jnp.float32) for target in targets] + [share_ref[...], spare]
    plan_ref[...] = jnp.concatenate(plan, axis=0).T
    for first in range(0, experts * slots, rows):
        place_here = row + first
        chosen = (place_here == targets[0]) | (place_here == targets[1])
        outgoing_ref[first : first + rows] = jnp.dot(
            chosen.astype(jnp.bfloat16), after, preferred_element_type=jnp.float32
        ).astype(jnp.bfloat16)


def mixer(index, ids, share, x, rim, gain, weight, scale, experts, side):
    rows = x.shape[0]
    col_count = weight.shape[1]
    slots = rows // ROWS * CAP
    return pl.pallas_call(
        functools.partial(mixer_kernel, experts),
        out_shape=(
            jax.ShapeDtypeStruct((experts * slots, col_count), jnp.bfloat16),
            jax.ShapeDtypeStruct((rows, 8), jnp.float32),
            *[jax.ShapeDtypeStruct((rows // side, col_count), jnp.bfloat16)] * side,
        ),
        in_specs=[SCALARS, VECTORS, VECTORS, FAR] + [VECTORS] * 4,
        out_specs=(VECTORS,) * (2 + side),
        scratch_shapes=[
            pltpu.VMEM(x.shape, x.dtype),
            pltpu.VMEM((rows, col_count), jnp.bfloat16),
            pltpu.SemaphoreType.DMA((GROUPS,)),
        ],
        compiler_params=pltpu.CompilerParams(vmem_limit_bytes=16 * 2**20),
        cost_estimate=pl.CostEstimate(
            flops=10**9, bytes_accessed=4 * x.size, transcendentals=rows
        ),
        name="mixer",
    )(index, ids, share, x, rim, gain[None], weight, scale[None])


def combine_kernel(slots, index_ref, returned_ref, plan_ref, parts_ref, out_ref, total_ref):
    side = parts_ref.shape[0]
    rows, _ = total_ref.shape
    quarter = index_ref[4]
    plan = plan_ref[pl.ds(pl.multiple_of(quarter * rows, rows), rows)]
    experts, height = (returned_ref.shape[0], slots // side)
    slot = lax.broadcasted_iota(jnp.int32, (rows, experts * height), 1)
    chosen = []
    for k in range(TOP_K):
        target = plan[:, k : k + 1].astype(jnp.int32)
        target = target // slots * height + target % height
        chosen.append((slot == target).astype(jnp.bfloat16))
    for tile in range(side):
        piece = returned_ref[:, tile * height : (tile + 1) * height].reshape(-1, LANES)
        mix = 0.0
        for k in range(TOP_K):
            picked = jnp.dot(chosen[k], piece, preferred_element_type=jnp.float32)
            mix = mix + plan[:, TOP_K + k : TOP_K + k + 1] * picked
        total_ref[:, tile * LANES : (tile + 1) * LANES] = mix
    for step in range(side):
        column = (quarter + side - step) % side * LANES
        here = pl.ds(pl.multiple_of(column, LANES), LANES)
        total_ref[:, here] = parts_ref[step].astype(jnp.float32) + total_ref[:, here]
    out = total_ref[...].astype(jnp.bfloat16)
    for t in range(out_ref.shape[0]):
        out_ref[t] = out


def combine(index, returned, plan, parts, slots, copies):
    rows, width = (parts.shape[1], parts.shape[0] * LANES)
    return pl.pallas_call(
        functools.partial(combine_kernel, slots),
        out_shape=jax.ShapeDtypeStruct((copies, rows, width), jnp.bfloat16),
        in_specs=[SCALARS] + [VECTORS] * 3,
        out_specs=VECTORS,
        scratch_shapes=[pltpu.VMEM((rows, width), jnp.float32)],
        compiler_params=pltpu.CompilerParams(vmem_limit_bytes=16 * 2**20),
        cost_estimate=pl.CostEstimate(
            flops=4 * returned.size * rows, bytes_accessed=10**6, transcendentals=0
        ),
        name="combine",
    )(index, returned, plan, parts)


def assemble_kernel(side, pieces_ref, out_ref, semaphores):
    count, rows, width = pieces_ref.shape
    copies = []
    for spot in range(count):
        row, quarter = divmod(spot, side)
        target = out_ref.at[quarter * rows : (quarter + 1) * rows, row * width : (row + 1) * width]
        copies.append(pltpu.make_async_copy(pieces_ref.at[spot], target, semaphores.at[spot]))
    for copy in copies:
        copy.start()
    for copy in copies:
        copy.wait()


def assemble(pieces, side):
    count, rows, width = pieces.shape
    return pl.pallas_call(
        functools.partial(assemble_kernel, side),
        out_shape=jax.ShapeDtypeStruct((side * rows, side * width), pieces.dtype),
        in_specs=[VECTORS],
        out_specs=ANYWHERE,
        scratch_shapes=[pltpu.SemaphoreType.DMA((count,))],
        compiler_params=pltpu.CompilerParams(vmem_limit_bytes=4 * 2**20),
        name="assemble",
    )(pieces)


def layer(
    residual_in,
    mix_gain,
    pool_weight,
    pool_scale,
    ffn_gain,
    route_ids,
    route_weights,
    gate_weight,
    up_weight,
    down_weight,
):
    tp_count = lax.axis_size(TP)
    sp_count = lax.axis_size(SP)
    tp_index = lax.axis_index(TP)
    sp_index = lax.axis_index(SP)
    tok_count, width = residual_in.shape
    col_count = pool_weight.shape[1]
    slots = tok_count // ROWS * CAP
    group_index = tp_index * col_count * GROUPS // width

    middle = up_weight.shape[2] // 2
    up_t = up_weight[0].T
    top = jnp.concatenate([gate_weight[0].T, up_t[:middle]], axis=0)
    bottom = jnp.concatenate([up_t[middle:], down_weight[0]], axis=0)
    left_top, right_bottom = (from_quad(top, 1), from_quad(bottom, -1))
    left_bottom, right_top = (from_quad(bottom, 1), from_quad(top, -1))
    rim = from_behind(residual_in[tok_count - SPAN :], SP, 1)

    side = lax.axis_size("x")
    core = lax.axis_index("c").astype(jnp.int32)
    column = lax.axis_index("x")
    place_in_quad = jnp.where(core == 0, column, lax.axis_index("y"))
    index = jnp.stack([group_index, tp_index, sp_index, column, place_in_quad]).astype(jnp.int32)
    core = core.reshape(1)
    outgoing, plan, *parts = mixer(
        index,
        route_ids.T,
        route_weights.T,
        residual_in,
        rim,
        mix_gain,
        pool_weight,
        pool_scale,
        sp_count,
        side,
    )
    outgoing = outgoing.reshape(sp_count, slots, col_count)
    arrived = lax.all_to_all(outgoing, SP, 0, 0, tiled=True)
    far_top, far_bottom = (from_quad(left_top, 1), from_quad(right_bottom, -1))

    parts = [from_mate(part, steps) for steps, part in enumerate(parts)]
    parts = jnp.stack(parts)
    quarter = jnp.moveaxis(arrived.reshape(sp_count, side, -1, col_count), 1, 0)
    quarter = jnp.broadcast_to(quarter[None], (side, *quarter.shape))
    gathered = exchange(quarter.reshape(tp_count, -1, col_count))
    term = expert(gathered, core, ffn_gain, [top, bottom, left_top, left_bottom, right_top, right_bottom, far_top, far_bottom], side)
    summed = exchange(term.reshape(side, side, -1, col_count), across=True)
    expert_out = jnp.sum(summed.astype(jnp.float32), axis=0).astype(jnp.bfloat16)
    expert_out = jnp.moveaxis(expert_out.reshape(side, sp_count, -1, col_count), 0, 1)
    expert_out = expert_out.reshape(sp_count, slots, col_count)
    returned = come_back(expert_out)
    copies = combine(index, returned, plan, parts, slots, tp_count)
    return assemble(exchange(copies), side)


def solution(mesh):
    torus = Mesh(mesh.devices.reshape(-1, 2, 4, mesh.shape["tp"] // 4), ALL)
    return jax.shard_map(
        layer,
        mesh=torus,
        in_specs=(
            P(SP, None),
            P(),
            P(None, TP),
            P(TP),
            P(),
            P(SP, None),
            P(SP, None),
            P(SP, None, TP),
            P(SP, None, TP),
            P(SP, TP, None),
        ),
        out_specs=P(SP, None),
        check_vma=False,
    )
```

```python
import functools
import math

import jax
import jax.numpy as jnp
import numpy as np
from jax import lax
from jax.experimental import pallas as pl
from jax.experimental.pallas import tpu as pltpu
from jax.sharding import Mesh
from jax.sharding import PartitionSpec as P

GROUPS = 4
SPAN = 16
TOP_K = 2
ROWS = 16
CAP = 2
SP = ("z", "c")
TP = ("y", "x")
ALL = ("z", "c", "y", "x")

EPS = 1e-06
LANES = 128


def from_behind(value, axis, steps):
    count = lax.axis_size(axis)
    first, last = (max(0, -steps), min(count, count - steps))
    return lax.ppermute(value, axis, [(source, source + steps) for source in range(first, last)])


def planes():
    sizes = [lax.axis_size(a) for a in ALL]
    index = np.arange(math.prod(sizes)).reshape(sizes)
    return [
        index[z, c] if c % 2 == 0 else index[z, c].T
        for z in range(sizes[0])
        for c in range(sizes[1])
    ]


def from_quad(value, steps):
    pairs = []
    for plane in planes():
        pairs += list(zip(plane.ravel().tolist(), np.roll(plane, -steps, axis=1).ravel().tolist()))
    return lax.ppermute(value, ALL, pairs)


def from_mate(value, steps):
    sizes = [lax.axis_size(a) for a in ALL]
    index = np.arange(math.prod(sizes)).reshape(sizes)
    pairs = []
    for number, plane in enumerate(planes()):
        owners = index[number // sizes[1], number % sizes[1]]
        pairs += list(zip(np.roll(owners, steps, axis=1).ravel().tolist(), plane.ravel().tolist()))
    return lax.ppermute(value, ALL, pairs)


def exchange(blocks, across=False):
    if across:
        groups = [column for plane in planes() for column in plane.T.tolist()]
    else:
        groups = [plane.ravel().tolist() for plane in planes()]
    return lax.all_to_all(blocks, ALL, 0, 0, tiled=True, axis_index_groups=groups)


def come_back(blocks):
    groups = np.stack([plane.ravel() for plane in planes()], axis=1).tolist()
    return lax.all_to_all(blocks, ALL, 0, 0, tiled=True, axis_index_groups=groups)


def place(t, side, swapped):
    return jnp.where(swapped == 0, t, (t % side) * side + t // side)


def expert_kernel(side, core_ref, x_ref, gain_ref, *refs):
    pieces = (len(refs) - 3) // 3 * 2
    sources, out_ref, normed_ref = (refs[:pieces], refs[pieces], refs[pieces + 1])
    weights, semaphores = (refs[pieces + 2 : -1], refs[-1])
    copies = []
    for i, source in enumerate(sources):
        height = source.shape[0]
        target = weights[i // 2].at[i % 2 * height : (i % 2 + 1) * height]
        copies.append(pltpu.make_async_copy(source, target, semaphores.at[i]))
    for copy in copies:
        copy.start()
    count, rows, lanes = x_ref.shape
    squares = jnp.zeros((rows, lanes), jnp.float32)
    for t in range(count):
        values = x_ref[t].astype(jnp.float32)
        squares = squares + values * values
    inverse = lax.rsqrt(jnp.sum(squares, axis=1, keepdims=True) / (count * lanes) + EPS)
    for t in range(count):
        columns = slice(t * lanes, (t + 1) * lanes)
        values = x_ref[place(t, side, core_ref[0])].astype(jnp.float32)
        normed_ref[:, columns] = (values * inverse * gain_ref[:, columns]).astype(jnp.bfloat16)
    units = weights[0].shape[0] // 3
    contract = (((1,), (1,)), ((), ()))
    normed = normed_ref[...]
    hidden, downs = ([], [])
    for i, ref in enumerate(weights):
        copies[2 * i].wait()
        copies[2 * i + 1].wait()
        gate_rows, up_rows = (ref[:units], ref[units : 2 * units])
        downs.append(ref.at[2 * units :])
        gate = lax.dot_general(normed, gate_rows, contract, preferred_element_type=jnp.float32)
        up = lax.dot_general(normed, up_rows, contract, preferred_element_type=jnp.float32)
        hidden.append((gate * (1.0 / (1.0 + jnp.exp(-gate))) * up).astype(jnp.bfloat16))
    for t in range(0, count, 2):
        total = 0.0
        for part, down in zip(hidden, downs):
            total = total + jnp.dot(
                part,
                down[:, t * lanes : (t + 2) * lanes],
                preferred_element_type=jnp.float32,
            )
        total = total.astype(jnp.bfloat16)
        out_ref[t] = total[:, :lanes]
        out_ref[t + 1] = total[:, lanes:]


SCALARS = pl.BlockSpec(memory_space=pltpu.SMEM)
VECTORS = pl.BlockSpec(memory_space=pltpu.VMEM)
ANYWHERE = pl.BlockSpec(memory_space=pl.ANY)
FAR = pl.BlockSpec(memory_space=pltpu.HBM)


def expert(blocks, core, gain, weights, side):
    count, rows, lanes = blocks.shape
    width = count * lanes
    slices = len(weights) // 2
    height = 2 * weights[0].shape[0]
    units = height // 3
    return pl.pallas_call(
        functools.partial(expert_kernel, side),
        out_shape=jax.ShapeDtypeStruct(blocks.shape, jnp.bfloat16),
        in_specs=[SCALARS, VECTORS, VECTORS] + [ANYWHERE] * len(weights),
        out_specs=VECTORS,
        scratch_shapes=[pltpu.VMEM((rows, width), jnp.bfloat16)]
        + [pltpu.VMEM((height, width), jnp.bfloat16)] * slices
        + [pltpu.SemaphoreType.DMA((len(weights),))],
        compiler_params=pltpu.CompilerParams(vmem_limit_bytes=32 * 2**20),
        cost_estimate=pl.CostEstimate(
            flops=6 * rows * units * width * side,
            bytes_accessed=6 * units * width * side,
            transcendentals=rows * units * side,
        ),
        name="expert",
    )(core, blocks, gain[None], *weights)


def inverse_rms(ref, copies=()):
    rows, width = ref.shape
    squares = jnp.zeros((rows, LANES), jnp.float32)
    for first in range(0, width, LANES):
        if copies and first % (width // len(copies)) == 0:
            copies[first * len(copies) // width].wait()
        values = ref[:, first : first + LANES].astype(jnp.float32)
        squares = squares + values * values
    return lax.rsqrt(jnp.sum(squares, axis=1, keepdims=True) / width + EPS)


def mixer_kernel(
    experts,
    index_ref,
    ids_ref,
    share_ref,
    source_ref,
    rim_ref,
    gain_ref,
    weight_ref,
    scale_ref,
    outgoing_ref,
    plan_ref,
    *refs,
):
    part_refs, (x_ref, after_ref, semaphores) = (refs[:-3], refs[-3:])
    copies = []
    part = source_ref.shape[1] // semaphores.shape[0]
    for i in range(semaphores.shape[0]):
        columns = slice(i * part, (i + 1) * part)
        copies.append(
            pltpu.make_async_copy(source_ref.at[:, columns], x_ref.at[:, columns], semaphores.at[i])
        )
    for copy in copies:
        copy.start()
    group, tp_index, sp_index = (index_ref[0], index_ref[1], index_ref[2])
    rows = x_ref.shape[0]
    span = rim_ref.shape[0]
    group_width, col_count = weight_ref.shape
    columns = pl.ds(pl.multiple_of(group * group_width, group_width), group_width)
    gain = gain_ref[:, columns]

    def normed(ref, inverse):
        return (ref[:, columns].astype(jnp.float32) * inverse * gain).astype(jnp.bfloat16)

    window = jnp.left_shift(2, group)
    here = normed(x_ref, inverse_rms(x_ref, copies))
    row = lax.broadcasted_iota(jnp.int32, (rows, rows), 0)
    col = lax.broadcasted_iota(jnp.int32, (rows, rows), 1)
    band = ((col <= row) & (row - col < window)).astype(jnp.bfloat16)
    sums = jnp.dot(band, here, preferred_element_type=jnp.float32)
    behind = lax.broadcasted_iota(jnp.int32, (rows, span), 0) + span
    behind = behind - lax.broadcasted_iota(jnp.int32, (rows, span), 1)
    sums = sums + jnp.dot(
        (behind < window).astype(jnp.bfloat16), normed(rim_ref, inverse_rms(rim_ref)), preferred_element_type=jnp.float32
    )
    position = sp_index * rows + lax.broadcasted_iota(jnp.int32, (rows, 1), 0)
    divisor = jnp.minimum(position + 1, window).astype(jnp.float32)
    pooled = (sums / divisor - here.astype(jnp.float32)).astype(jnp.bfloat16)
    mixed = jnp.dot(pooled, weight_ref[...], preferred_element_type=jnp.float32) * scale_ref[...]
    own = pl.ds(pl.multiple_of(tp_index * col_count, col_count), col_count)
    stream = x_ref[:, own].astype(jnp.float32)
    after = (stream + mixed.astype(jnp.bfloat16).astype(jnp.float32)).astype(jnp.bfloat16)
    after_ref[...] = after
    height = rows // len(part_refs)
    for step, ref in enumerate(part_refs):
        quarter = (index_ref[3] + step) % len(part_refs)
        ref[...] = after_ref[pl.ds(pl.multiple_of(quarter * height, height), height)]

    ids = ids_ref[...]
    expert_index = lax.broadcasted_iota(jnp.int32, (experts, rows), 0)
    named = [(ids[k : k + 1] == expert_index).astype(jnp.float32) for k in range(TOP_K)]
    earlier = ((row // ROWS == col // ROWS) & (row < col)).astype(jnp.bfloat16)
    before = jnp.dot(
        sum(named).astype(jnp.bfloat16), earlier, preferred_element_type=jnp.float32
    )
    slots = rows // ROWS * CAP
    block = lax.broadcasted_iota(jnp.int32, (1, rows), 1) // ROWS * CAP
    targets = []
    for k in range(TOP_K):
        slot = jnp.sum(before * named[k], axis=0, keepdims=True).astype(jnp.int32)
        targets.append(ids[k : k + 1] * slots + block + slot)
    spare = jnp.zeros((8 - 2 * TOP_K, rows), jnp.float32)
    plan = [target.astype(jnp.float32) for target in targets] + [share_ref[...], spare]
    plan_ref[...] = jnp.concatenate(plan, axis=0).T
    for first in range(0, experts * slots, rows):
        place_here = row + first
        chosen = (place_here == targets[0]) | (place_here == targets[1])
        outgoing_ref[first : first + rows] = jnp.dot(
            chosen.astype(jnp.bfloat16), after, preferred_element_type=jnp.float32
        ).astype(jnp.bfloat16)


def mixer(index, ids, share, x, rim, gain, weight, scale, experts, side):
    rows = x.shape[0]
    col_count = weight.shape[1]
    slots = rows // ROWS * CAP
    return pl.pallas_call(
        functools.partial(mixer_kernel, experts),
        out_shape=(
            jax.ShapeDtypeStruct((experts * slots, col_count), jnp.bfloat16),
            jax.ShapeDtypeStruct((rows, 8), jnp.float32),
            *[jax.ShapeDtypeStruct((rows // side, col_count), jnp.bfloat16)] * side,
        ),
        in_specs=[SCALARS, VECTORS, VECTORS, FAR] + [VECTORS] * 4,
        out_specs=(VECTORS,) * (2 + side),
        scratch_shapes=[
            pltpu.VMEM(x.shape, x.dtype),
            pltpu.VMEM((rows, col_count), jnp.bfloat16),
            pltpu.SemaphoreType.DMA((GROUPS,)),
        ],
        compiler_params=pltpu.CompilerParams(vmem_limit_bytes=16 * 2**20),
        cost_estimate=pl.CostEstimate(
            flops=10**9, bytes_accessed=4 * x.size, transcendentals=rows
        ),
        name="mixer",
    )(index, ids, share, x, rim, gain[None], weight, scale[None])


def combine_kernel(slots, index_ref, returned_ref, plan_ref, *refs):
    part_refs, out_ref, total_ref = (refs[:-2], refs[-2], refs[-1])
    side = len(part_refs)
    rows, _ = total_ref.shape
    quarter = index_ref[4]
    plan = plan_ref[pl.ds(pl.multiple_of(quarter * rows, rows), rows)]
    experts, height = (returned_ref.shape[0], slots // side)
    slot = lax.broadcasted_iota(jnp.int32, (rows, experts * height), 1)
    chosen = []
    for k in range(TOP_K):
        target = plan[:, k : k + 1].astype(jnp.int32)
        target = target // slots * height + target % height
        chosen.append((slot == target).astype(jnp.bfloat16))
    for tile in range(side):
        piece = returned_ref[:, tile * height : (tile + 1) * height].reshape(-1, LANES)
        mix = 0.0
        for k in range(TOP_K):
            picked = jnp.dot(chosen[k], piece, preferred_element_type=jnp.float32)
            mix = mix + plan[:, TOP_K + k : TOP_K + k + 1] * picked
        total_ref[:, tile * LANES : (tile + 1) * LANES] = mix
    for step, ref in enumerate(part_refs):
        column = (quarter + side - step) % side * LANES
        here = pl.ds(pl.multiple_of(column, LANES), LANES)
        total_ref[:, here] = ref[...].astype(jnp.float32) + total_ref[:, here]
    out = total_ref[...].astype(jnp.bfloat16)
    for t in range(out_ref.shape[0]):
        out_ref[t] = out


def combine(index, returned, plan, parts, slots, copies):
    rows, width = (parts[0].shape[0], len(parts) * LANES)
    return pl.pallas_call(
        functools.partial(combine_kernel, slots),
        out_shape=jax.ShapeDtypeStruct((copies, rows, width), jnp.bfloat16),
        in_specs=[SCALARS] + [VECTORS] * (2 + len(parts)),
        out_specs=VECTORS,
        scratch_shapes=[pltpu.VMEM((rows, width), jnp.float32)],
        compiler_params=pltpu.CompilerParams(vmem_limit_bytes=16 * 2**20),
        cost_estimate=pl.CostEstimate(
            flops=4 * returned.size * rows, bytes_accessed=10**6, transcendentals=0
        ),
        name="combine",
    )(index, returned, plan, *parts)


def assemble_kernel(side, pieces_ref, out_ref, semaphores):
    count, rows, width = pieces_ref.shape
    copies = []
    for spot in range(count):
        row, quarter = divmod(spot, side)
        target = out_ref.at[quarter * rows : (quarter + 1) * rows, row * width : (row + 1) * width]
        copies.append(pltpu.make_async_copy(pieces_ref.at[spot], target, semaphores.at[spot]))
    for copy in copies:
        copy.start()
    for copy in copies:
        copy.wait()


def assemble(pieces, side):
    count, rows, width = pieces.shape
    return pl.pallas_call(
        functools.partial(assemble_kernel, side),
        out_shape=jax.ShapeDtypeStruct((side * rows, side * width), pieces.dtype),
        in_specs=[VECTORS],
        out_specs=ANYWHERE,
        scratch_shapes=[pltpu.SemaphoreType.DMA((count,))],
        compiler_params=pltpu.CompilerParams(vmem_limit_bytes=4 * 2**20),
        name="assemble",
    )(pieces)


def layer(
    residual_in,
    mix_gain,
    pool_weight,
    pool_scale,
    ffn_gain,
    route_ids,
    route_weights,
    gate_weight,
    up_weight,
    down_weight,
):
    tp_count = lax.axis_size(TP)
    sp_count = lax.axis_size(SP)
    tp_index = lax.axis_index(TP)
    sp_index = lax.axis_index(SP)
    tok_count, width = residual_in.shape
    col_count = pool_weight.shape[1]
    slots = tok_count // ROWS * CAP
    group_index = tp_index * col_count * GROUPS // width

    middle = up_weight.shape[2] // 2
    up_t = up_weight[0].T
    top = jnp.concatenate([gate_weight[0].T, up_t[:middle]], axis=0)
    bottom = jnp.concatenate([up_t[middle:], down_weight[0]], axis=0)
    left_top, right_bottom = (from_quad(top, 1), from_quad(bottom, -1))
    left_bottom, right_top = (from_quad(bottom, 1), from_quad(top, -1))
    rim = from_behind(residual_in[tok_count - SPAN :], SP, 1)

    side = lax.axis_size("x")
    core = lax.axis_index("c").astype(jnp.int32)
    column = lax.axis_index("x")
    place_in_quad = jnp.where(core == 0, column, lax.axis_index("y"))
    index = jnp.stack([group_index, tp_index, sp_index, column, place_in_quad]).astype(jnp.int32)
    core = core.reshape(1)
    outgoing, plan, *parts = mixer(
        index,
        route_ids.T,
        route_weights.T,
        residual_in,
        rim,
        mix_gain,
        pool_weight,
        pool_scale,
        sp_count,
        side,
    )
    outgoing = outgoing.reshape(sp_count, slots, col_count)
    arrived = lax.all_to_all(outgoing, SP, 0, 0, tiled=True)
    far_top, far_bottom = (from_quad(left_top, 1), from_quad(right_bottom, -1))

    arrived_parts = [from_mate(parts[steps], steps) for steps in (0, 1)]
    parts = arrived_parts + [from_mate(parts[steps], steps) for steps in (2, 3)]
    quarter = jnp.moveaxis(arrived.reshape(sp_count, side, -1, col_count), 1, 0)
    quarter = jnp.broadcast_to(quarter[None], (side, *quarter.shape))
    gathered = exchange(quarter.reshape(tp_count, -1, col_count))
    term = expert(gathered, core, ffn_gain, [top, bottom, left_top, left_bottom, right_top, right_bottom, far_top, far_bottom], side)
    summed = exchange(term.reshape(side, side, -1, col_count), across=True)
    expert_out = jnp.sum(summed.astype(jnp.float32), axis=0).astype(jnp.bfloat16)
    expert_out = jnp.moveaxis(expert_out.reshape(side, sp_count, -1, col_count), 0, 1)
    expert_out = expert_out.reshape(sp_count, slots, col_count)
    returned = come_back(expert_out)
    copies = combine(index, returned, plan, parts, slots, tp_count)
    return assemble(exchange(copies), side)


def solution(mesh):
    torus = Mesh(mesh.devices.reshape(-1, 2, 4, mesh.shape["tp"] // 4), ALL)
    return jax.shard_map(
        layer,
        mesh=torus,
        in_specs=(
            P(SP, None),
            P(),
            P(None, TP),
            P(TP),
            P(),
            P(SP, None),
            P(SP, None),
            P(SP, None, TP),
            P(SP, None, TP),
            P(SP, TP, None),
        ),
        out_specs=P(SP, None),
        check_vma=False,
    )
```
